32 devices in a mesh: dp: 4 (over y, x), kv: 4 (over z), tp: 2 (over core).
Axes of the slice: x: 2, y: 2, z: 4, core: 2. Of those that a mesh axis runs over, the one named last changes fastest.
Arguments:
- token_state: bfloat16 [64, 4096], P('dp', 'kv'), may hold values from -150 to 150
- norm_gain: float32 [4096], P('kv'), may hold values from 0.1 to 1.9
- wq_nope: bfloat16 [4096, 1024], P('kv', 'tp'), may hold values from -0.09375 to 0.09375
- wq_rope: bfloat16 [4096, 512], P('kv', 'tp'), may hold values from -0.09375 to 0.09375
- w_latent: bfloat16 [4096, 512], P('kv'), may hold values from -0.09375 to 0.09375
- w_rope_key: bfloat16 [4096, 32], P('kv'), may hold values from -0.09375 to 0.09375
- kv_gain: float32 [512], replicated, may hold values from 0.1 to 1.9
- w_uk: bfloat16 [512, 1024], P('kv', 'tp'), may hold values from -0.25 to 0.25
- w_uv: bfloat16 [512, 1024], P('kv', 'tp'), may hold values from -6 to 6
- w_out: bfloat16 [1024, 4096], P('tp', 'kv'), may hold values from -0.1875 to 0.1875
- latent_cache: bfloat16 [64, 768, 512], P('dp', 'kv'), may hold values from -500 to 500
- rope_cache: bfloat16 [64, 32, 768], P('dp', None, 'kv'), may hold values from -6 to 6
- lengths: int32 [64], P('dp'), may hold values from 192 to 767, as said below
Outputs:
- mixed: bfloat16 [64, 4096], P('dp', ('kv', 'tp'))
- latent_new: bfloat16 [64, 512], P('dp')
- rope_new: bfloat16 [64, 32], P('dp')
The draws below stay inside these ranges and needn't reach their ends.
Inputs may be any that keep to these rules, and one draw needn't show every extreme that they name: Sequence b has cached positions 0 to lengths[b] - 1 and its new token takes position lengths[b]; in each aligned block of 16 sequences one has length 767.
All inputs are finite; a program needn't handle non-finite values.
Results may differ from the reference program's by a relative error of at most 0.02.
Values may be sent and summed in bfloat16 or wider, within the bound.
A program may use at most 64 MiB of HBM per device.

```python
import jax
import jax.numpy as jnp
from jax import lax

D = 4096
HEADS = 16
NOPE = 64
ROPE = 32
V_DIM = 64
RANK = 512
SEQS_DEV = 16
BATCH = 64
POSITIONS = 768
N_TP = 2


def draw_token_state(key, part):
    columns = jnp.arange(D, dtype=jnp.float32) / D
    col_scale = jnp.exp(jnp.log(5.0) * columns)
    sample = jnp.clip(jax.random.normal(key, (BATCH, D), jnp.float32), -6.0, 6.0)
    return (sample * col_scale[None, :]).astype(jnp.bfloat16)


def draw_latent_cache(key, part):
    shape = (BATCH, POSITIONS, RANK)
    sample = jnp.clip(jax.random.normal(key, shape, jnp.float32), -6.0, 6.0)
    return sample.astype(jnp.bfloat16)


def draw_lengths(key, part):
    groups = BATCH // SEQS_DEV
    sample = jax.random.randint(key, (groups, SEQS_DEV), POSITIONS // 4, POSITIONS)
    chosen = jax.random.randint(jax.random.fold_in(key, 1), (groups, 1), 0, SEQS_DEV)
    slots = jnp.arange(SEQS_DEV, dtype=jnp.int32)[None, :]
    sample = jnp.where(slots == chosen, POSITIONS - 1, sample)
    return sample.reshape(BATCH).astype(jnp.int32)


def level_of(rng, shape, cuts, low, high):
    level = 1.0
    for axis_at, shards_of in cuts:
        steps = jax.random.uniform(jax.random.fold_in(jax.random.fold_in(rng, 6), axis_at), (shards_of,), jnp.float32, low / len(cuts), high / len(cuts))
        level = level * jnp.repeat(jnp.exp(steps), shape[axis_at] // shards_of).reshape((-1,) + (1,) * (len(shape) - 1 - axis_at))
    return level


def centred(stream_key, dims, width, most, cuts=(), held_as=jnp.bfloat16):
    gain = level_of(stream_key, dims, cuts, -0.22, 0.18) if cuts else 1.0
    array = jax.random.normal(stream_key, dims, jnp.float32) * width * gain
    return jnp.minimum(jnp.maximum(array, -most), most).astype(held_as)


def setup_inputs(seed: int = 0) -> dict:
    key_list = jax.random.split(jax.random.key(seed), 14)
    return {
        "token_state": draw_token_state(jax.random.fold_in(key_list[13], 71), 0),
        "norm_gain": jnp.clip(1.0 + 0.18 * jax.random.normal(key_list[1], (D,), jnp.float32), 0.1, 1.9),
        "wq_nope": centred(key_list[2], (D, HEADS * NOPE), D ** -0.5, 0.09375, ((0, 4), (1, 2))),
        "wq_rope": centred(key_list[3], (D, HEADS * ROPE), D ** -0.5, 0.09375, ((0, 4), (1, 2))),
        "w_latent": centred(key_list[4], (D, RANK), D ** -0.5, 0.09375, ((0, 4),)),
        "w_rope_key": centred(key_list[5], (D, ROPE), D ** -0.5, 0.09375, ((0, 4),)),
        "kv_gain": jnp.clip(1.0 + 0.18 * jax.random.normal(key_list[6], (RANK,), jnp.float32), 0.1, 1.9),
        "w_uk": centred(key_list[7], (RANK, HEADS * NOPE), RANK ** -0.5, 0.25, ((0, 4), (1, 2))),
        "w_uv": centred(key_list[8], (RANK, HEADS * V_DIM), (0.25 * (POSITIONS // 256 + 1) ** 0.5), 6.0, ((0, 4), (1, 2))),
        "w_out": centred(key_list[9], (HEADS * V_DIM, D), (HEADS * V_DIM) ** -0.5, 0.1875, ((0, 2), (1, 4))),
        "latent_cache": draw_latent_cache(jax.random.fold_in(key_list[13], 71), 0),
        "rope_cache": centred(key_list[11], (BATCH, ROPE, POSITIONS), 1.0, 6.0, ((0, 4), (2, 4))),
        "lengths": draw_lengths(jax.random.fold_in(key_list[13], 71), 0),
    }


EPS = 1e-06
THETA = 10000.0
NEG = -1e+30

def rotate(vector, angles):
    half_dim = vector.shape[-1] // 2
    cosine = jnp.cos(angles)
    sine_part = jnp.sin(angles)
    leading = vector[..., :half_dim]
    trailing = vector[..., half_dim:]
    return jnp.concatenate([leading * cosine - trailing * sine_part, trailing * cosine + leading * sine_part], axis=-1)

def rope_angles(lengths):
    half_dim = ROPE // 2
    inv_freq = THETA ** (-jnp.arange(half_dim, dtype=jnp.float32) * 2.0 / ROPE)
    return lengths.astype(jnp.float32)[:, None] * inv_freq[None, :]

def reference(token_state, norm_gain, wq_nope, wq_rope, w_latent, w_rope_key, kv_gain, w_uk, w_uv, w_out, latent_cache, rope_cache, lengths):
    x_wide = token_state.astype(jnp.float32)
    inv_rms = lax.rsqrt(lax.optimization_barrier(jnp.sum(x_wide * x_wide, axis=1, keepdims=True)) / D + EPS)
    scaled = (x_wide * norm_gain).astype(jnp.bfloat16)
    q_nope = jnp.dot(scaled, wq_nope, preferred_element_type=jnp.float32) * inv_rms
    q_rope = jnp.dot(scaled, wq_rope, preferred_element_type=jnp.float32) * inv_rms
    latent_raw = jnp.dot(scaled, w_latent, preferred_element_type=jnp.float32) * inv_rms
    key_raw = jnp.dot(scaled, w_rope_key, preferred_element_type=jnp.float32) * inv_rms
    latent_new = (latent_raw * lax.rsqrt(lax.optimization_barrier(jnp.mean(latent_raw * latent_raw, axis=1, keepdims=True)) + EPS) * kv_gain).astype(jnp.bfloat16)
    angles = rope_angles(lengths)
    rope_new = rotate(key_raw, angles).astype(jnp.bfloat16)
    q_rot = rotate(q_rope.reshape(BATCH, HEADS, ROPE), angles[:, None, :]).astype(jnp.bfloat16)
    q_low = q_nope.astype(jnp.bfloat16).reshape(BATCH, HEADS, NOPE)
    q_latent = jnp.einsum('bhn,rhn->bhr', lax.optimization_barrier(q_low).astype(jnp.float32), w_uk.reshape(RANK, HEADS, NOPE).astype(jnp.float32)).astype(jnp.bfloat16)
    score_scale = (NOPE + ROPE) ** (-0.5)
    positions = jnp.arange(POSITIONS, dtype=jnp.int32)

    def per_sequence(items):
        query_lat, query_rot, latents, rope_rows, new_lat, new_rope, limit = items
        cached = jnp.dot(query_lat, latents.T, preferred_element_type=jnp.float32) + jnp.dot(query_rot, rope_rows, preferred_element_type=jnp.float32)
        own = jnp.dot(query_lat, new_lat[:, None], preferred_element_type=jnp.float32)[:, 0] + jnp.dot(query_rot, new_rope[:, None], preferred_element_type=jnp.float32)[:, 0]
        is_valid = positions < limit
        masked = jnp.where(is_valid[None, :], cached * score_scale, NEG)
        own = own * score_scale
        highest = jnp.maximum(lax.optimization_barrier(jnp.max(masked, axis=1)), own)
        weights = jnp.where(is_valid[None, :], jnp.exp(masked - highest[:, None]), 0.0)
        own_weight = jnp.exp(own - highest)
        totals = lax.optimization_barrier(jnp.sum(weights, axis=1)) + own_weight
        own_low = lax.optimization_barrier(own_weight.astype(jnp.bfloat16)).astype(jnp.float32)
        weighted = jnp.dot(weights.astype(jnp.bfloat16), latents, preferred_element_type=jnp.float32) + own_low[:, None] * new_lat.astype(jnp.float32)[None, :]
        return (weighted, totals)
    weighted, totals = lax.map(per_sequence, (q_latent, q_rot, latent_cache, rope_cache, latent_new, rope_new, lengths))
    weighted_low = lax.optimization_barrier(weighted.astype(jnp.bfloat16)).astype(jnp.float32)
    values = jnp.einsum('bhr,rhv->bhv', weighted_low, w_uv.reshape(RANK, HEADS, V_DIM).astype(jnp.float32)) / totals[:, :, None]
    attended = values.astype(jnp.bfloat16).reshape(BATCH, HEADS * V_DIM)
    group = HEADS * V_DIM // N_TP
    mixed = jnp.zeros((BATCH, D), jnp.float32)
    for index in range(N_TP):
        partial_out = jnp.dot(attended[:, index * group:(index + 1) * group], w_out[index * group:(index + 1) * group], preferred_element_type=jnp.float32)
        mixed = mixed + lax.optimization_barrier(partial_out.astype(jnp.bfloat16)).astype(jnp.float32)
    return (mixed.astype(jnp.bfloat16), latent_new, rope_new)
```

```python
import functools

import jax
import jax.numpy as jnp
import numpy as np
from jax import lax
from jax.experimental import pallas as pl
from jax.experimental.pallas import tpu as pltpu
from jax.sharding import PartitionSpec as P

D = 4096
NOPE = 64
ROPE = 32
V_DIM = 64


EPS = 1e-06
THETA = 10000.0
NEG = -1e30
LANES = 128
MESH = pl.DeviceIdType.MESH
BF16 = jnp.bfloat16
F32 = jnp.float32


def rotate(vector, angles):
    half_dim = vector.shape[-1] // 2
    cosine = jnp.cos(angles)
    sine_part = jnp.sin(angles)
    leading = vector[..., :half_dim]
    trailing = vector[..., half_dim:]
    return jnp.concatenate(
        [leading * cosine - trailing * sine_part, trailing * cosine + leading * sine_part], axis=-1
    )


def rope_angles(lengths):
    half_dim = ROPE // 2
    inv_freq = THETA ** (-jnp.arange(half_dim, dtype=jnp.float32) * 2.0 / ROPE)
    return lengths.astype(jnp.float32)[:, None] * inv_freq[None, :]


def dot_nt(a, b):
    return lax.dot_general(a, b, (((1,), (1,)), ((), ())), preferred_element_type=F32)


def dot(a, b):
    return jnp.dot(a, b, preferred_element_type=F32)


def swap_halves(u):
    width = u.shape[1]
    half = ROPE // 2
    lane = lax.broadcasted_iota(jnp.int32, u.shape, 1)
    from_above = pltpu.roll(u, width - half, 1)
    from_below = pltpu.roll(u, half, 1)
    return jnp.where(lane % ROPE < half, -from_above, from_below)


def per_head(u, heads, width):
    seqs, cols = u.shape
    wide = jnp.broadcast_to(u[:, None, :], (seqs, heads, cols))
    head = lax.broadcasted_iota(jnp.int32, wide.shape, 1)
    lane = lax.broadcasted_iota(jnp.int32, wide.shape, 2)
    return jnp.where(lane // width == head, wide, 0.0).reshape(seqs * heads, cols)


def kernel(
    n_kv,
    n_tp,
    len_ref,
    freq_ref,
    x_hbm,
    gain_hbm,
    wqn_hbm,
    wqr_hbm,
    wl_hbm,
    wk_hbm,
    kvg_hbm,
    wuk_hbm,
    wuv_hbm,
    wo_hbm,
    cache_hbm,
    rope_hbm,
    mixed_ref,
    lnew_ref,
    rnew_ref,
    x,
    gain,
    wqn,
    wqr,
    wl,
    wk,
    kvg,
    wuk,
    wuv,
    wo,
    cache,
    rope,
    part_q,
    part_l,
    part_v,
    half_out,
    half_in,
    scores,
    load_sem,
    send_sem,
    recv_sem,
    tp_sem,
):
    me = lax.axis_index("kv")
    core = lax.axis_index("tp")
    seqs = x.shape[0]
    heads = wqn.shape[1] // NOPE
    rank = wl.shape[1]
    nope_cols = wqn.shape[1]
    rope_cols = wqr.shape[1]
    block = cache.shape[1]
    rows = wuk_hbm.shape[0]

    pairs = (
        (x_hbm, x),
        (gain_hbm, gain),
        (wqn_hbm, wqn),
        (wqr_hbm, wqr),
        (wk_hbm, wk),
        (wl_hbm, wl),
        (kvg_hbm, kvg),
        (wuk_hbm, wuk.at[me]),
        (rope_hbm, rope),
        (cache_hbm, cache),
        (wuv_hbm, wuv.at[me]),
        (wo_hbm, wo),
    )
    loads = [pltpu.make_async_copy(s, d, load_sem.at[i]) for i, (s, d) in enumerate(pairs)]
    for load in loads:
        load.start()

    barrier = pltpu.get_barrier_semaphore()
    for j in range(1, n_kv):
        pl.semaphore_signal(
            barrier, inc=1, device_id={"kv": lax.rem(me + j, n_kv)}, device_id_type=MESH
        )
    for j in range(1, n_tp):
        pl.semaphore_signal(
            barrier, inc=1, device_id={"tp": lax.rem(core + j, n_tp)}, device_id_type=MESH
        )
    pl.semaphore_wait(barrier, n_kv - 1 + n_tp - 1)

    def copies(phase, src, dst):
        return [
            pltpu.make_async_remote_copy(
                src_ref=src,
                dst_ref=dst.at[me],
                send_sem=send_sem.at[phase, j - 1],
                recv_sem=recv_sem.at[phase, me],
                device_id={"kv": lax.rem(me + j, n_kv)},
                device_id_type=MESH,
            )
            for j in range(1, n_kv)
        ]

    def arrive(phase, dst):
        for j in range(1, n_kv):
            source = lax.rem(me + j, n_kv)
            pltpu.make_async_remote_copy(
                src_ref=dst.at[source],
                dst_ref=dst.at[source],
                send_sem=send_sem.at[phase, j - 1],
                recv_sem=recv_sem.at[phase, source],
                device_id={"kv": source},
                device_id_type=MESH,
            ).wait_recv()

    sent = []

    def send(phase, src, dst):
        group = copies(phase, src, dst)
        for c in group:
            c.start()
        sent.extend(group)

    send(0, wuk_hbm, wuk)

    loads[0].wait()
    loads[1].wait()
    x_wide = x[...].astype(F32)
    scaled = (x_wide * gain[...]).astype(BF16)
    squares = jnp.sum(x_wide * x_wide, axis=1, keepdims=True)
    loads[2].wait()
    part_q[me, :, :nope_cols] = dot(scaled, wqn[...])
    loads[3].wait()
    part_q[me, :, nope_cols : nope_cols + rope_cols] = dot(scaled, wqr[...])
    loads[4].wait()
    tail = slice(nope_cols + rope_cols, nope_cols + rope_cols + LANES)
    part_q[me, :, tail] = jnp.broadcast_to(squares, (seqs, LANES))
    part_q[me, :, nope_cols + rope_cols : nope_cols + rope_cols + ROPE] = dot(scaled, wk[...])
    send(1, part_q.at[me], part_q)
    loads[5].wait()
    part_l[me] = dot(scaled, wl[...])
    send(2, part_l.at[me], part_l)
    send(3, wuv_hbm, wuv)

    row = lax.broadcasted_iota(jnp.int32, (seqs, rope_cols), 0)
    length_rows = jnp.zeros((seqs, rope_cols), jnp.int32)
    for b in range(seqs):
        length_rows = jnp.where(row == b, len_ref[b], length_rows)
    angles = length_rows.astype(F32) * freq_ref[...]
    cosine = jnp.cos(angles)
    sine = jnp.sin(angles)

    arrive(1, part_q)
    total_q = part_q[0]
    for s in range(1, n_kv):
        total_q = total_q + part_q[s]
    last = total_q[:, tail]
    inv_rms = lax.rsqrt(last[:, ROPE : ROPE + 1] / D + EPS)
    q_low = (total_q[:, :nope_cols] * inv_rms).astype(BF16).astype(F32)
    q_rope = total_q[:, nope_cols : nope_cols + rope_cols] * inv_rms
    q_rot = (q_rope * cosine + swap_halves(q_rope) * sine).astype(BF16).astype(F32)
    key_raw = last * inv_rms
    rope_new = key_raw * cosine[:, :LANES] + swap_halves(key_raw) * sine[:, :LANES]
    rope_new = rope_new.astype(BF16)
    rnew_ref[...] = rope_new[:, :ROPE]

    q_blocks = per_head(q_low, heads, NOPE).astype(BF16)
    r_blocks = per_head(q_rot, heads, ROPE).astype(BF16)
    pick = (
        lax.broadcasted_iota(jnp.int32, (rope_cols, LANES), 0) % ROPE
        == lax.broadcasted_iota(jnp.int32, (rope_cols, LANES), 1)
    )
    q_rot_rows = dot(r_blocks, jnp.where(pick, 1.0, 0.0).astype(BF16))

    loads[7].wait()
    arrive(0, wuk)
    q_latent = jnp.concatenate(
        [dot_nt(q_blocks, wuk[s]) for s in range(n_kv)], axis=1
    ).astype(BF16).astype(F32)

    loads[8].wait()
    loads[9].wait()
    for b in range(seqs):
        at = slice(b * heads, (b + 1) * heads)
        scores[at, :] = dot_nt(q_latent[at].astype(BF16), cache[b]) + dot(
            q_rot_rows[at, :ROPE].astype(BF16), rope[b]
        )

    loads[6].wait()
    arrive(2, part_l)
    total_l = part_l[0]
    for s in range(1, n_kv):
        total_l = total_l + part_l[s]
    latent_raw = total_l * inv_rms
    mean_square = jnp.mean(latent_raw * latent_raw, axis=1, keepdims=True)
    latent_new = (latent_raw * lax.rsqrt(mean_square + EPS) * kvg[...]).astype(BF16)
    lnew_ref[...] = latent_new

    def rows_of(u):
        return jnp.broadcast_to(u[:, None, :], (seqs, heads, u.shape[1])).reshape(
            seqs * heads, u.shape[1]
        )

    new_rows = rows_of(latent_new.astype(F32))
    key_rows = rows_of(rope_new.astype(F32))
    own = jnp.sum(q_latent * new_rows, axis=1, keepdims=True)
    own = own + jnp.sum(q_rot_rows * key_rows, axis=1, keepdims=True)

    score_scale = (NOPE + ROPE) ** (-0.5)
    limit = jnp.concatenate(
        [jnp.full((heads, block), len_ref[b], jnp.int32) for b in range(seqs)], axis=0
    )
    place = me * block + lax.broadcasted_iota(jnp.int32, (seqs * heads, block), 1)
    newslot = place == limit
    usable = place <= limit
    masked = jnp.where(usable, jnp.where(newslot, own, scores[...]) * score_scale, NEG)
    local_max = jnp.max(masked, axis=1, keepdims=True)
    weights = jnp.where(usable, jnp.exp(masked - local_max), 0.0)
    totals = jnp.sum(weights, axis=1, keepdims=True)
    rounded = weights.astype(BF16).astype(F32)
    own_weight = jnp.sum(jnp.where(newslot, rounded, 0.0), axis=1, keepdims=True)
    cache_weights = jnp.where(newslot, 0.0, rounded)
    weighted = jnp.concatenate(
        [
            dot(cache_weights[b * heads : (b + 1) * heads].astype(BF16), cache[b])
            for b in range(seqs)
        ],
        axis=0,
    )
    weighted = (weighted + own_weight * new_rows).astype(BF16)

    loads[10].wait()
    arrive(3, wuv)
    values = dot(weighted[:, :rows], wuv[0])
    for s in range(1, n_kv):
        values = values + dot(weighted[:, s * rows : (s + 1) * rows], wuv[s])
    cols = values.shape[1]
    values = values.reshape(seqs, heads, cols)
    head = lax.broadcasted_iota(jnp.int32, values.shape, 1)
    lane = lax.broadcasted_iota(jnp.int32, values.shape, 2)
    part_v[me, :, :cols] = jnp.sum(jnp.where(lane // V_DIM == head, values, 0.0), axis=1)
    shape = (seqs, heads, LANES)
    head = lax.broadcasted_iota(jnp.int32, shape, 1)
    lane = lax.broadcasted_iota(jnp.int32, shape, 2)
    stats = jnp.where(
        lane == head, jnp.broadcast_to(local_max, (seqs * heads, LANES)).reshape(shape), 0.0
    ) + jnp.where(
        lane == head + LANES // 2,
        jnp.broadcast_to(totals, (seqs * heads, LANES)).reshape(shape),
        0.0,
    )
    part_v[me, :, cols:] = jnp.sum(stats, axis=1)
    send(4, part_v.at[me], part_v)
    arrive(4, part_v)

    maxima = [part_v[s, :, cols:] for s in range(n_kv)]
    sums = [pltpu.roll(m, LANES // 2, 1) for m in maxima]
    highest = functools.reduce(jnp.maximum, maxima)
    factors = [jnp.exp(m - highest) for m in maxima]
    whole = functools.reduce(jnp.add, [f * t for f, t in zip(factors, sums)])
    lane = lax.broadcasted_iota(jnp.int32, (seqs, cols), 1)

    def spread(u):
        out = jnp.broadcast_to(u[:, :1], (seqs, cols))
        for h in range(1, heads):
            out = jnp.where(lane // V_DIM == h, u[:, h : h + 1], out)
        return out

    merged = part_v[0, :, :cols] * spread(factors[0])
    for s in range(1, n_kv):
        merged = merged + part_v[s, :, :cols] * spread(factors[s])
    attended = (merged / spread(whole)).astype(BF16)

    loads[11].wait()
    width = half_in.shape[1]
    other = lax.rem(core + 1, n_tp)
    half_out[...] = dot(attended, wo[:, pl.ds(pl.multiple_of(other * width, width), width)]).astype(
        BF16
    )
    swap = pltpu.make_async_remote_copy(
        src_ref=half_out,
        dst_ref=half_in,
        send_sem=tp_sem.at[0],
        recv_sem=tp_sem.at[1],
        device_id={"tp": other},
        device_id_type=MESH,
    )
    swap.start()
    mine = dot(attended, wo[:, pl.ds(pl.multiple_of(core * width, width), width)]).astype(BF16)
    swap.wait()
    mixed_ref[...] = (mine.astype(F32) + half_in[...].astype(F32)).astype(BF16)
    for c in sent:
        c.wait_send()


def fused(n_kv, n_tp, *args):
    (x, gain, wqn, wqr, wl, wk, kvg, wuk, wuv, wo, cache, rope, lengths) = args
    seqs, rank = x.shape[0], wl.shape[1]
    heads = wqn.shape[1] // NOPE
    q_cols = wqn.shape[1] + wqr.shape[1] + LANES
    half = wo.shape[1] // n_tp
    freq = THETA ** (-(np.arange(wqr.shape[1]) % (ROPE // 2)) * 2.0 / ROPE)
    freq = jnp.asarray(freq.astype(np.float32)[None, :])
    any_spec = pl.BlockSpec(memory_space=pl.ANY)
    vmem = pl.BlockSpec(memory_space=pltpu.VMEM)

    def like(a, *lead):
        return pltpu.VMEM(tuple(lead) + a.shape, a.dtype)

    gain = gain.reshape(1, -1)
    kvg = kvg.reshape(1, -1)
    return pl.pallas_call(
        functools.partial(kernel, n_kv, n_tp),
        out_shape=(
            jax.ShapeDtypeStruct((seqs, half), BF16),
            jax.ShapeDtypeStruct((seqs, rank), BF16),
            jax.ShapeDtypeStruct((seqs, ROPE), BF16),
        ),
        in_specs=[pl.BlockSpec(memory_space=pltpu.SMEM), vmem] + [any_spec] * 12,
        out_specs=(vmem, vmem, vmem),
        scratch_shapes=[
            like(x),
            like(gain),
            like(wqn),
            like(wqr),
            like(wl),
            like(wk),
            like(kvg),
            like(wuk, n_kv),
            like(wuv, n_kv),
            like(wo),
            like(cache),
            like(rope),
            pltpu.VMEM((n_kv, seqs, q_cols), F32),
            pltpu.VMEM((n_kv, seqs, rank), F32),
            pltpu.VMEM((n_kv, seqs, wuv.shape[1] + LANES), F32),
            pltpu.VMEM((seqs, half), BF16),
            pltpu.VMEM((seqs, half), BF16),
            pltpu.VMEM((seqs * heads, cache.shape[1]), F32),
            pltpu.SemaphoreType.DMA((12,)),
            pltpu.SemaphoreType.DMA((5, n_kv - 1)),
            pltpu.SemaphoreType.DMA((5, n_kv)),
            pltpu.SemaphoreType.DMA((2,)),
        ],
        compiler_params=pltpu.CompilerParams(collective_id=0, has_side_effects=True),
    )(lengths, freq, x, gain, wqn, wqr, wl, wk, kvg, wuk, wuv, wo, cache, rope)


def local(
    token_state,
    norm_gain,
    wq_nope,
    wq_rope,
    w_latent,
    w_rope_key,
    kv_gain,
    w_uk,
    w_uv,
    w_out,
    latent_cache,
    rope_cache,
    lengths,
):
    x_wide = token_state.astype(jnp.float32)
    scaled = (x_wide * norm_gain).astype(jnp.bfloat16)
    partials = (
        jnp.sum(x_wide * x_wide, axis=1),
        jnp.dot(scaled, wq_nope, preferred_element_type=jnp.float32),
        jnp.dot(scaled, wq_rope, preferred_element_type=jnp.float32),
        jnp.dot(scaled, w_latent, preferred_element_type=jnp.float32),
        jnp.dot(scaled, w_rope_key, preferred_element_type=jnp.float32),
    )
    squares, nope_sum, rope_sum, latent_sum, key_sum = lax.psum(
        (partials[0], partials[1], partials[2], partials[3], partials[4]), "kv"
    )
    inv_rms = lax.rsqrt(squares / D + EPS)[:, None]
    seq_count = token_state.shape[0]
    head_count = wq_nope.shape[1] // NOPE
    latent_raw = latent_sum * inv_rms
    latent_new = (
        latent_raw
        * lax.rsqrt(jnp.mean(latent_raw * latent_raw, axis=1, keepdims=True) + EPS)
        * kv_gain
    ).astype(jnp.bfloat16)
    angles = rope_angles(lengths)
    rope_new = rotate(key_sum * inv_rms, angles).astype(jnp.bfloat16)
    q_rot = rotate(
        (rope_sum * inv_rms).reshape(seq_count, head_count, ROPE), angles[:, None, :]
    ).astype(jnp.bfloat16)
    q_low = (nope_sum * inv_rms).astype(jnp.bfloat16).reshape(seq_count, head_count, NOPE)
    row_count = w_uk.shape[0]
    q_piece = jnp.einsum(
        "bhn,rhn->bhr",
        q_low,
        w_uk.reshape(row_count, head_count, NOPE),
        preferred_element_type=jnp.float32,
    ).astype(jnp.bfloat16)
    q_latent = lax.all_gather(q_piece, "kv", axis=2, tiled=True)
    block_len = latent_cache.shape[1]
    positions = lax.axis_index("kv") * block_len + jnp.arange(block_len, dtype=jnp.int32)
    score_scale = (NOPE + ROPE) ** (-0.5)
    cached = jnp.einsum("bhr,bpr->bhp", q_latent, latent_cache, preferred_element_type=jnp.float32)
    cached = cached + jnp.einsum(
        "bhk,bkp->bhp", q_rot, rope_cache, preferred_element_type=jnp.float32
    )
    own = jnp.einsum("bhr,br->bh", q_latent, latent_new, preferred_element_type=jnp.float32)
    own = own + jnp.einsum("bhk,bk->bh", q_rot, rope_new, preferred_element_type=jnp.float32)
    limit = lengths[:, None, None]
    newslot = positions[None, None, :] == limit
    usable = (positions[None, None, :] < limit) | newslot
    scores = jnp.where(newslot, own[:, :, None], cached) * score_scale
    masked = jnp.where(usable, scores, NEG)
    local_max = jnp.max(masked, axis=2)
    weights = jnp.where(usable, jnp.exp(masked - local_max[..., None]), 0.0)
    totals = jnp.sum(weights, axis=2)
    rounded = weights.astype(jnp.bfloat16)
    cache_weights = jnp.where(newslot, jnp.zeros_like(rounded), rounded)
    weighted = jnp.einsum(
        "bhp,bpr->bhr", cache_weights, latent_cache, preferred_element_type=jnp.float32
    )
    own_low = lax.optimization_barrier(jnp.where(newslot, rounded, jnp.zeros_like(rounded)))
    own_weight = jnp.sum(own_low.astype(jnp.float32), axis=2)
    weighted = weighted + own_weight[..., None] * latent_new.astype(jnp.float32)[:, None, :]
    value_rows = w_uv.shape[0]
    w_values = w_uv.reshape(value_rows, head_count, V_DIM)
    highest = lax.pmax(local_max, "kv")
    factor = jnp.exp(local_max - highest)
    latent_piece = lax.psum_scatter(
        weighted * factor[..., None], "kv", scatter_dimension=2, tiled=True
    ).astype(jnp.bfloat16)
    partial_values = jnp.einsum(
        "bhr,rhv->bhv", latent_piece, w_values, preferred_element_type=jnp.float32
    )
    value_sum, totals = lax.psum((partial_values, totals * factor), "kv")
    values = value_sum / totals[:, :, None]
    attended = values.astype(jnp.bfloat16).reshape(seq_count, head_count * V_DIM)
    out_term = jnp.dot(attended, w_out, preferred_element_type=jnp.float32)
    mixed = lax.psum_scatter(out_term.astype(jnp.bfloat16), "tp", scatter_dimension=1, tiled=True)
    return (mixed, latent_new, rope_new)


def solution(mesh):
    n_kv, n_tp = mesh.shape["kv"], mesh.shape["tp"]

    def body(*args):
        width, rank = args[9].shape[1], args[4].shape[1]
        if (width // n_tp) % LANES == 0 and (rank // n_kv) % LANES == 0:
            return fused(n_kv, n_tp, *args)
        return local(*args)

    return jax.shard_map(
        body,
        mesh=mesh,
        in_specs=(
            P("dp", "kv"),
            P("kv"),
            P("kv", "tp"),
            P("kv", "tp"),
            P("kv", None),
            P("kv", None),
            P(),
            P("kv", "tp"),
            P("kv", "tp"),
            P("tp", "kv"),
            P("dp", "kv", None),
            P("dp", None, "kv"),
            P("dp"),
        ),
        out_specs=(P("dp", ("kv", "tp")), P("dp", None), P("dp", None)),
        check_vma=False,
    )
```

```python
import functools

import jax
import jax.numpy as jnp
import numpy as np
from jax import lax
from jax.experimental import pallas as pl
from jax.experimental.pallas import tpu as pltpu
from jax.sharding import PartitionSpec as P

D = 4096
NOPE = 64
ROPE = 32
V_DIM = 64


EPS = 1e-06
THETA = 10000.0
NEG = -1e30
LANES = 128
MESH = pl.DeviceIdType.MESH
BF16 = jnp.bfloat16
F32 = jnp.float32


def rotate(vector, angles):
    half_dim = vector.shape[-1] // 2
    cosine = jnp.cos(angles)
    sine_part = jnp.sin(angles)
    leading = vector[..., :half_dim]
    trailing = vector[..., half_dim:]
    return jnp.concatenate(
        [leading * cosine - trailing * sine_part, trailing * cosine + leading * sine_part], axis=-1
    )


def rope_angles(lengths):
    half_dim = ROPE // 2
    inv_freq = THETA ** (-jnp.arange(half_dim, dtype=jnp.float32) * 2.0 / ROPE)
    return lengths.astype(jnp.float32)[:, None] * inv_freq[None, :]


def dot_nt(a, b):
    return lax.dot_general(a, b, (((1,), (1,)), ((), ())), preferred_element_type=F32)


def dot(a, b):
    return jnp.dot(a, b, preferred_element_type=F32)


def swap_halves(u):
    width = u.shape[1]
    half = ROPE // 2
    lane = lax.broadcasted_iota(jnp.int32, u.shape, 1)
    from_above = pltpu.roll(u, width - half, 1)
    from_below = pltpu.roll(u, half, 1)
    return jnp.where(lane % ROPE < half, -from_above, from_below)


def kernel(
    n_dp,
    n_kv,
    n_tp,
    len_ref,
    freq_ref,
    x_hbm,
    gain_hbm,
    wqn_hbm,
    wqr_hbm,
    wl_hbm,
    wk_hbm,
    kvg_hbm,
    wuk_hbm,
    wuv_hbm,
    wo_hbm,
    cache_hbm,
    rope_hbm,
    mixed_ref,
    lnew_ref,
    rnew_ref,
    x,
    gain,
    wqn,
    wqr,
    wl,
    wk,
    kvg,
    wuk,
    wuv,
    wo,
    cache,
    rope,
    key_pad,
    q_out,
    q_in,
    lat_in,
    lat_half,
    q_lat,
    q_rots,
    val_in,
    stat_in,
    half_out,
    half_in,
    scores,
    load_sem,
    send_sem,
    recv_sem,
    dp_send,
    dp_recv,
    tp_sem,
):
    me = lax.axis_index("kv")
    core = lax.axis_index("tp")
    group = lax.axis_index("dp")
    seqs = x.shape[0]
    heads = wqn.shape[1] // NOPE
    own_heads = heads // n_kv
    rank = kvg.shape[1]
    lat_cols = wl.shape[1]
    block = cache.shape[1]
    rows = wuv_hbm.shape[0]
    part = rows // n_dp

    def cols(index, width):
        return pl.ds(pl.multiple_of(index * width, width), width)

    part_rows = cols(group, part)
    pairs = (
        (x_hbm, x),
        (gain_hbm, gain),
        (wqn_hbm, wqn),
        (wqr_hbm, wqr),
        (wk_hbm, wk),
        (wl_hbm.at[:, cols(core, lat_cols)], wl),
        (kvg_hbm, kvg),
        (wuk_hbm.at[:, cols(me, LANES)], wuk.at[me]),
        (rope_hbm, rope),
        (cache_hbm, cache),
        (wuv_hbm, wuv.at[me]),
        (wo_hbm, wo),
    )
    loads = [pltpu.make_async_copy(s, d, load_sem.at[i]) for i, (s, d) in enumerate(pairs)]
    for load in loads:
        load.start()

    barrier = pltpu.get_barrier_semaphore()
    axes = (("kv", me, n_kv), ("tp", core, n_tp), ("dp", group, n_dp))
    for name, index, size in axes:
        for j in range(1, size):
            pl.semaphore_signal(
                barrier, inc=1, device_id={name: lax.rem(index + j, size)}, device_id_type=MESH
            )
    pl.semaphore_wait(barrier, n_kv - 1 + n_tp - 1 + n_dp - 1)

    sent = []

    def send(phase, src, dst):
        for j in range(1, n_kv):
            peer = lax.rem(me + j, n_kv)
            copy = pltpu.make_async_remote_copy(
                src_ref=src(peer),
                dst_ref=dst(me),
                send_sem=send_sem.at[phase, j - 1],
                recv_sem=recv_sem.at[phase, me],
                device_id={"kv": peer},
                device_id_type=MESH,
            )
            copy.start()
            sent.append(copy)

    def arrive(phase, dst):
        for j in range(1, n_kv):
            source = lax.rem(me + j, n_kv)
            pltpu.make_async_remote_copy(
                src_ref=dst(source),
                dst_ref=dst(source),
                send_sem=send_sem.at[phase, j - 1],
                recv_sem=recv_sem.at[phase, source],
                device_id={"kv": source},
                device_id_type=MESH,
            ).wait_recv()

    send(0, lambda p: wuk_hbm.at[:, cols(p, LANES)], lambda s: wuk.at[s])

    loads[0].wait()
    loads[1].wait()
    x_wide = x[...].astype(F32)
    scaled = (x_wide * gain[...]).astype(BF16)
    squares = jnp.sum(x_wide * x_wide, axis=1, keepdims=True)
    key_pad[...] = jnp.broadcast_to(squares, key_pad.shape)
    loads[4].wait()
    key_pad[:, :ROPE] = dot_nt(scaled, wk[...])
    rope_own = own_heads * ROPE
    key_part = pltpu.roll(key_pad[...], rope_own, 1)
    loads[2].wait()
    nope_part = dot(scaled, wqn[...])
    loads[3].wait()
    rope_part = dot(scaled, wqr[...])
    lane = lax.broadcasted_iota(jnp.int32, (seqs, LANES), 1)
    for s in range(n_kv):
        q_out[s, :, :LANES] = nope_part[:, s * LANES : (s + 1) * LANES]
        first, shift = divmod(s * rope_own, LANES)
        piece = rope_part[:, first * LANES : (first + 1) * LANES]
        if shift:
            piece = pltpu.roll(piece, LANES - shift, 1)
        q_out[s, :, LANES:] = jnp.where(lane < rope_own, piece, key_part)
    send(1, lambda p: q_out.at[p], lambda s: q_in.at[s])
    q_in[me] = q_out[me]
    send(2, lambda p: wuv_hbm.at[part_rows], lambda s: wuv.at[s, part_rows])
    loads[5].wait()
    lat_in[me] = dot(scaled, wl[...])
    send(3, lambda p: lat_in.at[me], lambda s: lat_in.at[s])

    row = lax.broadcasted_iota(jnp.int32, (seqs, LANES), 0)
    length_rows = jnp.zeros((seqs, LANES), jnp.int32)
    for b in range(seqs):
        length_rows = jnp.where(row == b, len_ref[b], length_rows)
    angles = length_rows.astype(F32) * freq_ref[...]
    cosine = jnp.cos(angles)
    sine = jnp.sin(angles)

    arrive(1, lambda s: q_in.at[s])
    total_q = q_in[0]
    for s in range(1, n_kv):
        total_q = total_q + q_in[s]
    last = total_q[:, LANES:]
    inv_rms = lax.rsqrt(last[:, LANES - 1 :] / D + EPS)
    q_low = total_q[:, :LANES] * inv_rms
    last = last * inv_rms
    turned = (last * cosine + swap_halves(last) * sine).astype(BF16)
    q_rots[me] = turned
    send(4, lambda p: q_rots.at[me], lambda s: q_rots.at[s])
    q_blocks = jnp.concatenate(
        [jnp.where(lane // NOPE == h, q_low, 0.0) for h in range(own_heads)], axis=0
    ).astype(BF16)
    loads[7].wait()
    arrive(0, lambda s: wuk.at[s])
    for s in range(n_kv):
        q_lat[me, :, s * rows : (s + 1) * rows] = dot_nt(q_blocks, wuk[s]).astype(BF16)
    send(5, lambda p: q_lat.at[me], lambda s: q_lat.at[s])
    rope_new = pltpu.roll(turned.astype(F32), LANES - rope_own, 1)
    rnew_ref[...] = rope_new[:, :ROPE].astype(BF16)

    arrive(2, lambda s: wuv.at[s, part_rows])
    for j in range(1, n_dp):
        peer = lax.rem(group + j, n_dp)
        for i in range(1, n_kv):
            source = lax.rem(me + i, n_kv)
            copy = pltpu.make_async_remote_copy(
                src_ref=wuv.at[source, part_rows],
                dst_ref=wuv.at[source, part_rows],
                send_sem=dp_send.at[j - 1, i - 1],
                recv_sem=dp_recv.at[group, i - 1],
                device_id={"dp": peer},
                device_id_type=MESH,
            )
            copy.start()
            sent.append(copy)

    arrive(3, lambda s: lat_in.at[s])
    total_l = lat_in[0]
    for s in range(1, n_kv):
        total_l = total_l + lat_in[s]
    lat_half[core] = total_l
    other = lax.rem(core + 1, n_tp)
    lat_swap = pltpu.make_async_remote_copy(
        src_ref=lat_half.at[core],
        dst_ref=lat_half.at[core],
        send_sem=tp_sem.at[0],
        recv_sem=tp_sem.at[1],
        device_id={"tp": other},
        device_id_type=MESH,
    )
    lat_swap.start()

    count = seqs * heads
    to = lax.broadcasted_iota(jnp.int32, (count, count), 0)
    frm = lax.broadcasted_iota(jnp.int32, (count, count), 1)
    order = jnp.where(frm == (to % heads) * seqs + to // heads, 1.0, 0.0).astype(BF16)
    arrive(4, lambda s: q_rots.at[s])
    wide = jnp.concatenate([q_rots[s] for s in range(n_kv)], axis=1).astype(F32)
    shape = (seqs, heads, n_kv * LANES)
    head = lax.broadcasted_iota(jnp.int32, shape, 1)
    at = lax.broadcasted_iota(jnp.int32, shape, 2)
    mine = (at // LANES == head // own_heads) & ((at % LANES) // ROPE == head % own_heads)
    r_blocks = jnp.where(mine, jnp.broadcast_to(wide[:, None, :], shape), 0.0)
    r_blocks = r_blocks.reshape(count, n_kv * LANES).astype(BF16)
    pick_shape = (n_kv * LANES, LANES)
    pick = (
        lax.broadcasted_iota(jnp.int32, pick_shape, 0) % ROPE
        == lax.broadcasted_iota(jnp.int32, pick_shape, 1)
    )
    q_rot_rows = dot(r_blocks, jnp.where(pick, 1.0, 0.0).astype(BF16))
    arrive(5, lambda s: q_lat.at[s])
    q_latent = dot(order, q_lat[...].reshape(count, rank))

    loads[8].wait()
    loads[9].wait()
    for b in range(seqs):
        span = slice(b * heads, (b + 1) * heads)
        scores[span, :] = dot_nt(q_latent[span].astype(BF16), cache[b]) + dot(
            q_rot_rows[span, :ROPE].astype(BF16), rope[b]
        )

    loads[6].wait()
    lat_swap.wait()
    latent_raw = jnp.concatenate([lat_half[t] for t in range(n_tp)], axis=1) * inv_rms
    mean_square = jnp.mean(latent_raw * latent_raw, axis=1, keepdims=True)
    latent_new = (latent_raw * lax.rsqrt(mean_square + EPS) * kvg[...]).astype(BF16)
    lnew_ref[...] = latent_new

    def rows_of(u):
        return jnp.broadcast_to(u[:, None, :], (seqs, heads, u.shape[1])).reshape(
            count, u.shape[1]
        )

    new_rows = rows_of(latent_new.astype(F32))
    key_rows = rows_of(rope_new)
    own = jnp.sum(q_latent * new_rows, axis=1, keepdims=True)
    own = own + jnp.sum(q_rot_rows * key_rows, axis=1, keepdims=True)

    score_scale = (NOPE + ROPE) ** (-0.5)
    limit = jnp.concatenate(
        [jnp.full((heads, block), len_ref[b], jnp.int32) for b in range(seqs)], axis=0
    )
    place = me * block + lax.broadcasted_iota(jnp.int32, (count, block), 1)
    newslot = place == limit
    usable = place <= limit
    masked = jnp.where(usable, jnp.where(newslot, own, scores[...]) * score_scale, NEG)
    local_max = jnp.max(masked, axis=1, keepdims=True)
    weights = jnp.where(usable, jnp.exp(masked - local_max), 0.0)
    totals = jnp.sum(weights, axis=1, keepdims=True)
    rounded = weights.astype(BF16).astype(F32)
    own_weight = jnp.sum(jnp.where(newslot, rounded, 0.0), axis=1, keepdims=True)
    cache_weights = jnp.where(newslot, 0.0, rounded)
    weighted = jnp.concatenate(
        [
            dot(cache_weights[b * heads : (b + 1) * heads].astype(BF16), cache[b])
            for b in range(seqs)
        ],
        axis=0,
    )
    weighted = (weighted + own_weight * new_rows).astype(BF16)

    shape = (seqs, heads, LANES)
    head = lax.broadcasted_iota(jnp.int32, shape, 1)
    at = lax.broadcasted_iota(jnp.int32, shape, 2)
    stats = jnp.where(
        at == head, jnp.broadcast_to(local_max, (count, LANES)).reshape(shape), 0.0
    ) + jnp.where(
        at == head + LANES // 2, jnp.broadcast_to(totals, (count, LANES)).reshape(shape), 0.0
    )
    stat_in[me] = jnp.sum(stats, axis=1)
    send(6, lambda p: stat_in.at[me], lambda s: stat_in.at[s])
    loads[10].wait()
    for j in range(1, n_dp):
        source_group = lax.rem(group + j, n_dp)
        their_rows = cols(source_group, part)
        for i in range(1, n_kv):
            source = lax.rem(me + i, n_kv)
            pltpu.make_async_remote_copy(
                src_ref=wuv.at[source, their_rows],
                dst_ref=wuv.at[source, their_rows],
                send_sem=dp_send.at[j - 1, i - 1],
                recv_sem=dp_recv.at[source_group, i - 1],
                device_id={"dp": source_group},
                device_id_type=MESH,
            ).wait_recv()
    values = dot(weighted, wuv[...].reshape(rank, wuv.shape[2]))
    width = values.shape[1]
    values = values.reshape(seqs, heads, width)
    head = lax.broadcasted_iota(jnp.int32, values.shape, 1)
    at = lax.broadcasted_iota(jnp.int32, values.shape, 2)
    val_in[me] = jnp.sum(jnp.where(at // V_DIM == head, values, 0.0), axis=1).astype(BF16)
    send(7, lambda p: val_in.at[me], lambda s: val_in.at[s])

    arrive(6, lambda s: stat_in.at[s])
    maxima = [stat_in[s] for s in range(n_kv)]
    sums = [pltpu.roll(m, LANES // 2, 1) for m in maxima]
    highest = functools.reduce(jnp.maximum, maxima)
    factors = [jnp.exp(m - highest) for m in maxima]
    whole = functools.reduce(jnp.add, [f * t for f, t in zip(factors, sums)])
    at = lax.broadcasted_iota(jnp.int32, (seqs, width), 1)

    def spread(u):
        out = jnp.broadcast_to(u[:, :1], (seqs, width))
        for h in range(1, heads):
            out = jnp.where(at // V_DIM == h, u[:, h : h + 1], out)
        return out

    spreads = [spread(f) for f in factors]
    divisor = spread(whole)
    arrive(7, lambda s: val_in.at[s])
    merged = val_in[0].astype(F32) * spreads[0]
    for s in range(1, n_kv):
        merged = merged + val_in[s].astype(F32) * spreads[s]
    attended = (merged / divisor).astype(BF16)

    loads[11].wait()
    out_cols = half_in.shape[1]
    half_out[...] = dot(attended, wo[:, cols(other, out_cols)]).astype(BF16)
    swap = pltpu.make_async_remote_copy(
        src_ref=half_out,
        dst_ref=half_in,
        send_sem=tp_sem.at[2],
        recv_sem=tp_sem.at[3],
        device_id={"tp": other},
        device_id_type=MESH,
    )
    swap.start()
    kept = dot(attended, wo[:, cols(core, out_cols)]).astype(BF16)
    swap.wait()
    mixed_ref[...] = (kept.astype(F32) + half_in[...].astype(F32)).astype(BF16)
    for c in sent:
        c.wait_send()


def fused(n_dp, n_kv, n_tp, *args):
    (x, gain, wqn, wqr, wl, wk, kvg, wuk, wuv, wo, cache, rope, lengths) = args
    seqs, rank = x.shape[0], wl.shape[1]
    heads = wqn.shape[1] // NOPE
    half = wo.shape[1] // n_tp
    freq = THETA ** (-(np.arange(LANES) % (ROPE // 2)) * 2.0 / ROPE)
    freq = jnp.asarray(freq.astype(np.float32)[None, :])
    any_spec = pl.BlockSpec(memory_space=pl.ANY)
    vmem = pl.BlockSpec(memory_space=pltpu.VMEM)

    def like(a):
        return pltpu.VMEM(a.shape, a.dtype)

    gain = gain.reshape(1, -1)
    kvg = kvg.reshape(1, -1)
    wk = wk.T
    return pl.pallas_call(
        functools.partial(kernel, n_dp, n_kv, n_tp),
        out_shape=(
            jax.ShapeDtypeStruct((seqs, half), BF16),
            jax.ShapeDtypeStruct((seqs, rank), BF16),
            jax.ShapeDtypeStruct((seqs, ROPE), BF16),
        ),
        in_specs=[pl.BlockSpec(memory_space=pltpu.SMEM), vmem] + [any_spec] * 12,
        out_specs=(vmem, vmem, vmem),
        scratch_shapes=[
            like(x),
            like(gain),
            like(wqn),
            like(wqr),
            pltpu.VMEM((wl.shape[0], rank // n_tp), BF16),
            like(wk),
            like(kvg),
            pltpu.VMEM((n_kv, wuk.shape[0], LANES), BF16),
            pltpu.VMEM((n_kv,) + wuv.shape, BF16),
            like(wo),
            like(cache),
            like(rope),
            pltpu.VMEM((seqs, LANES), F32),
            pltpu.VMEM((n_kv, seqs, 2 * LANES), F32),
            pltpu.VMEM((n_kv, seqs, 2 * LANES), F32),
            pltpu.VMEM((n_kv, seqs, rank // n_tp), F32),
            pltpu.VMEM((n_tp, seqs, rank // n_tp), F32),
            pltpu.VMEM((n_kv, heads // n_kv * seqs, rank), BF16),
            pltpu.VMEM((n_kv, seqs, LANES), BF16),
            pltpu.VMEM((n_kv, seqs, wuv.shape[1]), BF16),
            pltpu.VMEM((n_kv, seqs, LANES), F32),
            pltpu.VMEM((seqs, half), BF16),
            pltpu.VMEM((seqs, half), BF16),
            pltpu.VMEM((seqs * heads, cache.shape[1]), F32),
            pltpu.SemaphoreType.DMA((12,)),
            pltpu.SemaphoreType.DMA((8, n_kv - 1)),
            pltpu.SemaphoreType.DMA((8, n_kv)),
            pltpu.SemaphoreType.DMA((n_dp - 1, n_kv - 1)),
            pltpu.SemaphoreType.DMA((n_dp, n_kv - 1)),
            pltpu.SemaphoreType.DMA((4,)),
        ],
        compiler_params=pltpu.CompilerParams(collective_id=0, has_side_effects=True),
    )(lengths, freq, x, gain, wqn, wqr, wl, wk, kvg, wuk, wuv, wo, cache, rope)


def local(
    token_state,
    norm_gain,
    wq_nope,
    wq_rope,
    w_latent,
    w_rope_key,
    kv_gain,
    w_uk,
    w_uv,
    w_out,
    latent_cache,
    rope_cache,
    lengths,
):
    x_wide = token_state.astype(jnp.float32)
    scaled = (x_wide * norm_gain).astype(jnp.bfloat16)
    partials = (
        jnp.sum(x_wide * x_wide, axis=1),
        jnp.dot(scaled, wq_nope, preferred_element_type=jnp.float32),
        jnp.dot(scaled, wq_rope, preferred_element_type=jnp.float32),
        jnp.dot(scaled, w_latent, preferred_element_type=jnp.float32),
        jnp.dot(scaled, w_rope_key, preferred_element_type=jnp.float32),
    )
    squares, nope_sum, rope_sum, latent_sum, key_sum = lax.psum(
        (partials[0], partials[1], partials[2], partials[3], partials[4]), "kv"
    )
    inv_rms = lax.rsqrt(squares / D + EPS)[:, None]
    seq_count = token_state.shape[0]
    head_count = wq_nope.shape[1] // NOPE
    latent_raw = latent_sum * inv_rms
    latent_new = (
        latent_raw
        * lax.rsqrt(jnp.mean(latent_raw * latent_raw, axis=1, keepdims=True) + EPS)
        * kv_gain
    ).astype(jnp.bfloat16)
    angles = rope_angles(lengths)
    rope_new = rotate(key_sum * inv_rms, angles).astype(jnp.bfloat16)
    q_rot = rotate(
        (rope_sum * inv_rms).reshape(seq_count, head_count, ROPE), angles[:, None, :]
    ).astype(jnp.bfloat16)
    q_low = (nope_sum * inv_rms).astype(jnp.bfloat16).reshape(seq_count, head_count, NOPE)
    row_count = w_uk.shape[0]
    q_piece = jnp.einsum(
        "bhn,rhn->bhr",
        q_low,
        w_uk.reshape(row_count, head_count, NOPE),
        preferred_element_type=jnp.float32,
    ).astype(jnp.bfloat16)
    q_latent = lax.all_gather(q_piece, "kv", axis=2, tiled=True)
    block_len = latent_cache.shape[1]
    positions = lax.axis_index("kv") * block_len + jnp.arange(block_len, dtype=jnp.int32)
    score_scale = (NOPE + ROPE) ** (-0.5)
    cached = jnp.einsum("bhr,bpr->bhp", q_latent, latent_cache, preferred_element_type=jnp.float32)
    cached = cached + jnp.einsum(
        "bhk,bkp->bhp", q_rot, rope_cache, preferred_element_type=jnp.float32
    )
    own = jnp.einsum("bhr,br->bh", q_latent, latent_new, preferred_element_type=jnp.float32)
    own = own + jnp.einsum("bhk,bk->bh", q_rot, rope_new, preferred_element_type=jnp.float32)
    limit = lengths[:, None, None]
    newslot = positions[None, None, :] == limit
    usable = (positions[None, None, :] < limit) | newslot
    scores = jnp.where(newslot, own[:, :, None], cached) * score_scale
    masked = jnp.where(usable, scores, NEG)
    local_max = jnp.max(masked, axis=2)
    weights = jnp.where(usable, jnp.exp(masked - local_max[..., None]), 0.0)
    totals = jnp.sum(weights, axis=2)
    rounded = weights.astype(jnp.bfloat16)
    cache_weights = jnp.where(newslot, jnp.zeros_like(rounded), rounded)
    weighted = jnp.einsum(
        "bhp,bpr->bhr", cache_weights, latent_cache, preferred_element_type=jnp.float32
    )
    own_low = lax.optimization_barrier(jnp.where(newslot, rounded, jnp.zeros_like(rounded)))
    own_weight = jnp.sum(own_low.astype(jnp.float32), axis=2)
    weighted = weighted + own_weight[..., None] * latent_new.astype(jnp.float32)[:, None, :]
    value_rows = w_uv.shape[0]
    w_values = w_uv.reshape(value_rows, head_count, V_DIM)
    highest = lax.pmax(local_max, "kv")
    factor = jnp.exp(local_max - highest)
    latent_piece = lax.psum_scatter(
        weighted * factor[..., None], "kv", scatter_dimension=2, tiled=True
    ).astype(jnp.bfloat16)
    partial_values = jnp.einsum(
        "bhr,rhv->bhv", latent_piece, w_values, preferred_element_type=jnp.float32
    )
    value_sum, totals = lax.psum((partial_values, totals * factor), "kv")
    values = value_sum / totals[:, :, None]
    attended = values.astype(jnp.bfloat16).reshape(seq_count, head_count * V_DIM)
    out_term = jnp.dot(attended, w_out, preferred_element_type=jnp.float32)
    mixed = lax.psum_scatter(out_term.astype(jnp.bfloat16), "tp", scatter_dimension=1, tiled=True)
    return (mixed, latent_new, rope_new)


def solution(mesh):
    n_dp, n_kv, n_tp = mesh.shape["dp"], mesh.shape["kv"], mesh.shape["tp"]

    def body(*args):
        width, rank = args[9].shape[1], args[4].shape[1]
        aligned = (width // n_tp) % LANES == 0 and (rank // n_kv) % LANES == 0
        if aligned and args[2].shape[1] == n_kv * LANES and n_tp == 2:
            return fused(n_dp, n_kv, n_tp, *args)
        return local(*args)

    return jax.shard_map(
        body,
        mesh=mesh,
        in_specs=(
            P("dp", "kv"),
            P("kv"),
            P("kv", "tp"),
            P("kv", "tp"),
            P("kv", None),
            P("kv", None),
            P(),
            P("kv", "tp"),
            P("kv", "tp"),
            P("tp", "kv"),
            P("dp", "kv", None),
            P("dp", None, "kv"),
            P("dp"),
        ),
        out_specs=(P("dp", ("kv", "tp")), P("dp", None), P("dp", None)),
        check_vma=False,
    )
```

```python
import functools

import jax
import jax.numpy as jnp
import numpy as np
from jax import lax
from jax.experimental import pallas as pl
from jax.experimental.pallas import tpu as pltpu
from jax.sharding import PartitionSpec as P

D = 4096
NOPE = 64
ROPE = 32
V_DIM = 64


EPS = 1e-06
THETA = 10000.0
NEG = -1e30
LANES = 128
CHUNKS = 2
MESH = pl.DeviceIdType.MESH
BF16 = jnp.bfloat16
F32 = jnp.float32


def rotate(vector, angles):
    half_dim = vector.shape[-1] // 2
    cosine = jnp.cos(angles)
    sine_part = jnp.sin(angles)
    leading = vector[..., :half_dim]
    trailing = vector[..., half_dim:]
    return jnp.concatenate(
        [leading * cosine - trailing * sine_part, trailing * cosine + leading * sine_part], axis=-1
    )


def rope_angles(lengths):
    half_dim = ROPE // 2
    inv_freq = THETA ** (-jnp.arange(half_dim, dtype=jnp.float32) * 2.0 / ROPE)
    return lengths.astype(jnp.float32)[:, None] * inv_freq[None, :]


def dot_nt(a, b):
    return lax.dot_general(a, b, (((1,), (1,)), ((), ())), preferred_element_type=F32)


def dot(a, b):
    return jnp.dot(a, b, preferred_element_type=F32)


def swap_halves(u):
    width = u.shape[1]
    half = ROPE // 2
    lane = lax.broadcasted_iota(jnp.int32, u.shape, 1)
    from_above = pltpu.roll(u, width - half, 1)
    from_below = pltpu.roll(u, half, 1)
    return jnp.where(lane % ROPE < half, -from_above, from_below)


def kernel(
    n_dp,
    n_kv,
    n_tp,
    len_ref,
    freq_ref,
    x_hbm,
    gain_hbm,
    wqn_hbm,
    wqr_hbm,
    wl_hbm,
    wk_hbm,
    kvg_hbm,
    wuk_hbm,
    wuv_hbm,
    wo_hbm,
    cache_hbm,
    rope_hbm,
    mixed_ref,
    lnew_ref,
    rnew_ref,
    x,
    gain,
    wqn,
    wqr,
    wl,
    wk,
    kvg,
    wuk,
    wuv,
    wo,
    cache,
    rope,
    key_pad,
    q_out,
    q_in,
    lat_in,
    lat_half,
    q_lat,
    q_rots,
    val_in,
    stat_in,
    half_out,
    half_in,
    scores,
    load_sem,
    send_sem,
    recv_sem,
    dp_send,
    dp_recv,
    tp_sem,
):
    me = lax.axis_index("kv")
    core = lax.axis_index("tp")
    group = lax.axis_index("dp")
    seqs = x.shape[0]
    heads = wqn.shape[1] // NOPE
    own_heads = heads // n_kv
    rank = kvg.shape[1]
    lat_cols = wl.shape[1]
    block = cache.shape[1]
    rows = wuv_hbm.shape[0]
    chunks = q_lat.shape[0]
    span = seqs // chunks
    count = span * heads
    part = rows // n_dp

    def cols(index, width):
        return pl.ds(pl.multiple_of(index * width, width), width)

    barrier = pltpu.get_barrier_semaphore()
    axes = (("kv", me, n_kv), ("tp", core, n_tp), ("dp", group, n_dp))
    for name, index, size in axes:
        for j in range(1, size):
            pl.semaphore_signal(
                barrier, inc=1, device_id={name: lax.rem(index + j, size)}, device_id_type=MESH
            )
    part_rows = cols(group, part)
    pairs = (
        (x_hbm, x),
        (gain_hbm, gain),
        (wqn_hbm, wqn),
        (wqr_hbm, wqr),
        (wk_hbm, wk),
        (wl_hbm.at[:, cols(core, lat_cols)], wl),
        (kvg_hbm, kvg),
        (wuk_hbm.at[:, cols(me, LANES)], wuk.at[me]),
        (rope_hbm, rope),
        (cache_hbm, cache),
        (wuv_hbm, wuv.at[me]),
        (wo_hbm, wo),
    )
    loads = [pltpu.make_async_copy(s, d, load_sem.at[i]) for i, (s, d) in enumerate(pairs)]
    for i in (0, 1, 4, 2, 3):
        loads[i].start()
    pl.semaphore_wait(barrier, n_kv - 1 + n_tp - 1 + n_dp - 1)

    sent = []

    def send(phase, src, dst):
        for j in range(1, n_kv):
            peer = lax.rem(me + j, n_kv)
            copy = pltpu.make_async_remote_copy(
                src_ref=src(peer),
                dst_ref=dst(me),
                send_sem=send_sem.at[phase, j - 1],
                recv_sem=recv_sem.at[phase, me],
                device_id={"kv": peer},
                device_id_type=MESH,
            )
            copy.start()
            sent.append(copy)

    def arrive(phase, dst):
        for j in range(1, n_kv):
            source = lax.rem(me + j, n_kv)
            pltpu.make_async_remote_copy(
                src_ref=dst(source),
                dst_ref=dst(source),
                send_sem=send_sem.at[phase, j - 1],
                recv_sem=recv_sem.at[phase, source],
                device_id={"kv": source},
                device_id_type=MESH,
            ).wait_recv()

    send(0, lambda p: wuk_hbm.at[:, cols(p, LANES)], lambda s: wuk.at[s])

    loads[0].wait()
    loads[1].wait()
    x_wide = x[...].astype(F32)
    scaled = (x_wide * gain[...]).astype(BF16)
    squares = jnp.sum(x_wide * x_wide, axis=1, keepdims=True)
    key_pad[...] = jnp.broadcast_to(squares, key_pad.shape)
    loads[4].wait()
    key_pad[:, :ROPE] = dot_nt(scaled, wk[...])
    rope_own = own_heads * ROPE
    key_part = pltpu.roll(key_pad[...], rope_own, 1)
    loads[2].wait()
    for i in (5, 7, 6, 8, 9, 10, 11):
        loads[i].start()
    nope_part = dot(scaled, wqn[...])
    loads[3].wait()
    rope_part = dot(scaled, wqr[...])
    lane = lax.broadcasted_iota(jnp.int32, (seqs, LANES), 1)
    for s in range(n_kv):
        q_out[s, :, :LANES] = nope_part[:, s * LANES : (s + 1) * LANES]
        first, shift = divmod(s * rope_own, LANES)
        piece = rope_part[:, first * LANES : (first + 1) * LANES]
        if shift:
            piece = pltpu.roll(piece, LANES - shift, 1)
        q_out[s, :, LANES:] = jnp.where(lane < rope_own, piece, key_part)
    send(1, lambda p: q_out.at[p], lambda s: q_in.at[s])
    q_in[me] = q_out[me]
    send(2, lambda p: wuv_hbm.at[part_rows], lambda s: wuv.at[s, part_rows])
    loads[5].wait()
    lat_in[me] = dot(scaled, wl[...])
    send(3, lambda p: lat_in.at[me], lambda s: lat_in.at[s])

    row = lax.broadcasted_iota(jnp.int32, (seqs, LANES), 0)
    length_rows = jnp.zeros((seqs, LANES), jnp.int32)
    for b in range(seqs):
        length_rows = jnp.where(row == b, len_ref[b], length_rows)
    angles = length_rows.astype(F32) * freq_ref[...]
    cosine = jnp.cos(angles)
    sine = jnp.sin(angles)

    arrive(1, lambda s: q_in.at[s])
    total_q = q_in[0]
    for s in range(1, n_kv):
        total_q = total_q + q_in[s]
    last = total_q[:, LANES:]
    inv_rms = lax.rsqrt(last[:, LANES - 1 :] / D + EPS)
    q_low = total_q[:, :LANES] * inv_rms
    last = last * inv_rms
    turned = (last * cosine + swap_halves(last) * sine).astype(BF16)
    q_rots[me] = turned
    send(4, lambda p: q_rots.at[me], lambda s: q_rots.at[s])
    q_blocks = jnp.concatenate(
        [
            jnp.where(lane[:span] // NOPE == h, q_low[c * span : (c + 1) * span], 0.0)
            for c in range(chunks)
            for h in range(own_heads)
        ],
        axis=0,
    ).astype(BF16)
    loads[7].wait()
    arrive(0, lambda s: wuk.at[s])
    per_chunk = own_heads * span
    for s in range(n_kv):
        piece = dot_nt(q_blocks, wuk[s]).astype(BF16)
        for c in range(chunks):
            q_lat[c, me, :, s * rows : (s + 1) * rows] = piece[c * per_chunk : (c + 1) * per_chunk]
    for c in range(chunks):
        send(5 + c, lambda p: q_lat.at[c, me], lambda s: q_lat.at[c, s])
    rope_new = pltpu.roll(turned.astype(F32), LANES - rope_own, 1)
    rnew_ref[...] = rope_new[:, :ROPE].astype(BF16)

    arrive(2, lambda s: wuv.at[s, part_rows])
    for j in range(1, n_dp):
        peer = lax.rem(group + j, n_dp)
        for i in range(1, n_kv):
            source = lax.rem(me + i, n_kv)
            copy = pltpu.make_async_remote_copy(
                src_ref=wuv.at[source, part_rows],
                dst_ref=wuv.at[source, part_rows],
                send_sem=dp_send.at[j - 1, i - 1],
                recv_sem=dp_recv.at[group, i - 1],
                device_id={"dp": peer},
                device_id_type=MESH,
            )
            copy.start()
            sent.append(copy)

    arrive(3, lambda s: lat_in.at[s])
    total_l = lat_in[0]
    for s in range(1, n_kv):
        total_l = total_l + lat_in[s]
    lat_half[core] = total_l
    other = lax.rem(core + 1, n_tp)
    lat_swap = pltpu.make_async_remote_copy(
        src_ref=lat_half.at[core],
        dst_ref=lat_half.at[core],
        send_sem=tp_sem.at[0],
        recv_sem=tp_sem.at[1],
        device_id={"tp": other},
        device_id_type=MESH,
    )
    lat_swap.start()

    arrive(4, lambda s: q_rots.at[s])
    wide = jnp.concatenate([q_rots[s] for s in range(n_kv)], axis=1).astype(F32)
    shape = (seqs, heads, n_kv * LANES)
    head = lax.broadcasted_iota(jnp.int32, shape, 1)
    at = lax.broadcasted_iota(jnp.int32, shape, 2)
    mine = (at // LANES == head // own_heads) & ((at % LANES) // ROPE == head % own_heads)
    r_blocks = jnp.where(mine, jnp.broadcast_to(wide[:, None, :], shape), 0.0)
    r_blocks = r_blocks.reshape(seqs * heads, n_kv * LANES).astype(BF16)
    pick_shape = (n_kv * LANES, LANES)
    pick = (
        lax.broadcasted_iota(jnp.int32, pick_shape, 0) % ROPE
        == lax.broadcasted_iota(jnp.int32, pick_shape, 1)
    )
    q_rot_rows = dot(r_blocks, jnp.where(pick, 1.0, 0.0).astype(BF16))

    to = lax.broadcasted_iota(jnp.int32, (count, count), 0)
    frm = lax.broadcasted_iota(jnp.int32, (count, count), 1)
    order = jnp.where(frm == (to % heads) * span + to // heads, 1.0, 0.0).astype(BF16)
    place = me * block + lax.broadcasted_iota(jnp.int32, (count, block), 1)
    score_scale = (NOPE + ROPE) ** (-0.5)
    stat_shape = (span, heads, LANES)
    stat_head = lax.broadcasted_iota(jnp.int32, stat_shape, 1)
    stat_lane = lax.broadcasted_iota(jnp.int32, stat_shape, 2)
    width = wuv.shape[2]
    val_shape = (span, heads, width)
    own_columns = lax.broadcasted_iota(jnp.int32, val_shape, 2) // V_DIM == (
        lax.broadcasted_iota(jnp.int32, val_shape, 1)
    )

    def rows_of(u):
        return jnp.broadcast_to(u[:, None, :], (span, heads, u.shape[1])).reshape(
            count, u.shape[1]
        )

    for c in range(chunks):
        first = c * span
        arrive(5 + c, lambda s: q_lat.at[c, s])
        q_latent = dot(order, q_lat[c].reshape(count, rank))
        q_turn = q_rot_rows[first * heads : (first + span) * heads]
        if c == 0:
            loads[8].wait()
            loads[9].wait()
        for b in range(span):
            some = slice(b * heads, (b + 1) * heads)
            scores[some, :] = dot_nt(q_latent[some].astype(BF16), cache[first + b]) + dot(
                q_turn[some, :ROPE].astype(BF16), rope[first + b]
            )
        if c == 0:
            loads[6].wait()
            lat_swap.wait()
            latent_raw = jnp.concatenate([lat_half[t] for t in range(n_tp)], axis=1) * inv_rms
            mean_square = jnp.mean(latent_raw * latent_raw, axis=1, keepdims=True)
            latent_new = latent_raw * lax.rsqrt(mean_square + EPS) * kvg[...]
            latent_new = latent_new.astype(BF16)
            lnew_ref[...] = latent_new
            latent_wide = latent_new.astype(F32)

        new_rows = rows_of(latent_wide[first : first + span])
        key_rows = rows_of(rope_new[first : first + span])
        own = jnp.sum(q_latent * new_rows, axis=1, keepdims=True)
        own = own + jnp.sum(q_turn * key_rows, axis=1, keepdims=True)

        limit = jnp.concatenate(
            [jnp.full((heads, block), len_ref[first + b], jnp.int32) for b in range(span)], axis=0
        )
        newslot = place == limit
        usable = place <= limit
        masked = jnp.where(usable, jnp.where(newslot, own, scores[...]) * score_scale, NEG)
        local_max = jnp.max(masked, axis=1, keepdims=True)
        weights = jnp.where(usable, jnp.exp(masked - local_max), 0.0)
        totals = jnp.sum(weights, axis=1, keepdims=True)
        rounded = weights.astype(BF16).astype(F32)
        own_weight = jnp.sum(jnp.where(newslot, rounded, 0.0), axis=1, keepdims=True)
        cache_weights = jnp.where(newslot, 0.0, rounded)
        stats = jnp.where(
            stat_lane == stat_head,
            jnp.broadcast_to(local_max, (count, LANES)).reshape(stat_shape),
            0.0,
        ) + jnp.where(
            stat_lane == stat_head + LANES // 2,
            jnp.broadcast_to(totals, (count, LANES)).reshape(stat_shape),
            0.0,
        )
        stat_in[c, me] = jnp.sum(stats, axis=1)
        send(7 + c, lambda p: stat_in.at[c, me], lambda s: stat_in.at[c, s])
        weighted = jnp.concatenate(
            [
                dot(cache_weights[b * heads : (b + 1) * heads].astype(BF16), cache[first + b])
                for b in range(span)
            ],
            axis=0,
        )
        weighted = (weighted + own_weight * new_rows).astype(BF16)

        if c == 0:
            loads[10].wait()
            for j in range(1, n_dp):
                source_group = lax.rem(group + j, n_dp)
                their_rows = cols(source_group, part)
                for i in range(1, n_kv):
                    source = lax.rem(me + i, n_kv)
                    pltpu.make_async_remote_copy(
                        src_ref=wuv.at[source, their_rows],
                        dst_ref=wuv.at[source, their_rows],
                        send_sem=dp_send.at[j - 1, i - 1],
                        recv_sem=dp_recv.at[source_group, i - 1],
                        device_id={"dp": source_group},
                        device_id_type=MESH,
                    ).wait_recv()
        values = dot(weighted, wuv[...].reshape(rank, width)).reshape(val_shape)
        val_in[c, me] = jnp.sum(jnp.where(own_columns, values, 0.0), axis=1).astype(BF16)
        send(9 + c, lambda p: val_in.at[c, me], lambda s: val_in.at[c, s])

    at = lax.broadcasted_iota(jnp.int32, (span, width), 1)

    def spread(u):
        out = jnp.broadcast_to(u[:, :1], (span, width))
        for h in range(1, heads):
            out = jnp.where(at // V_DIM == h, u[:, h : h + 1], out)
        return out

    merged_chunks = []
    for c in range(chunks):
        arrive(7 + c, lambda s: stat_in.at[c, s])
        maxima = [stat_in[c, s] for s in range(n_kv)]
        sums = [pltpu.roll(m, LANES // 2, 1) for m in maxima]
        highest = functools.reduce(jnp.maximum, maxima)
        factors = [jnp.exp(m - highest) for m in maxima]
        whole = functools.reduce(jnp.add, [f * t for f, t in zip(factors, sums)])
        spreads = [spread(f) for f in factors]
        divisor = spread(whole)
        arrive(9 + c, lambda s: val_in.at[c, s])
        merged = val_in[c, 0].astype(F32) * spreads[0]
        for s in range(1, n_kv):
            merged = merged + val_in[c, s].astype(F32) * spreads[s]
        merged_chunks.append(merged / divisor)
    attended = jnp.concatenate(merged_chunks, axis=0).astype(BF16)

    loads[11].wait()
    out_cols = half_in.shape[1]
    half_out[...] = dot(attended, wo[:, cols(other, out_cols)]).astype(BF16)
    swap = pltpu.make_async_remote_copy(
        src_ref=half_out,
        dst_ref=half_in,
        send_sem=tp_sem.at[2],
        recv_sem=tp_sem.at[3],
        device_id={"tp": other},
        device_id_type=MESH,
    )
    swap.start()
    kept = dot(attended, wo[:, cols(core, out_cols)]).astype(BF16)
    swap.wait()
    mixed_ref[...] = (kept.astype(F32) + half_in[...].astype(F32)).astype(BF16)
    for c in sent:
        c.wait_send()


def hand_out(*refs):
    n = (len(refs) - 1) // 3
    ins, outs, held, sem = refs[:n], refs[n : 2 * n], refs[2 * n : 3 * n], refs[-1]
    for step, (frm, to) in enumerate(((ins, held), (held, outs))):
        copies = [pltpu.make_async_copy(frm[i], to[i], sem.at[step, i]) for i in range(n)]
        for copy in copies:
            copy.start()
        for copy in copies:
            copy.wait()


def fused(n_dp, n_kv, n_tp, *args):
    (x, gain, wqn, wqr, wl, wk, kvg, wuk, wuv, wo, cache, rope, lengths) = args
    seqs, rank = x.shape[0], wl.shape[1]
    heads = wqn.shape[1] // NOPE
    half = wo.shape[1] // n_tp
    freq = THETA ** (-(np.arange(LANES) % (ROPE // 2)) * 2.0 / ROPE)
    freq = jnp.asarray(freq.astype(np.float32)[None, :])
    any_spec = pl.BlockSpec(memory_space=pl.ANY)
    vmem = pl.BlockSpec(memory_space=pltpu.VMEM)

    def like(a):
        return pltpu.VMEM(a.shape, a.dtype)

    gain = gain.reshape(1, -1)
    kvg = kvg.reshape(1, -1)
    wk = wk.T
    outs = pl.pallas_call(
        functools.partial(kernel, n_dp, n_kv, n_tp),
        out_shape=(
            jax.ShapeDtypeStruct((seqs, half), BF16),
            jax.ShapeDtypeStruct((seqs, rank), BF16),
            jax.ShapeDtypeStruct((seqs, ROPE), BF16),
        ),
        in_specs=[pl.BlockSpec(memory_space=pltpu.SMEM), vmem] + [any_spec] * 12,
        out_specs=(vmem, vmem, vmem),
        scratch_shapes=[
            like(x),
            like(gain),
            like(wqn),
            like(wqr),
            pltpu.VMEM((wl.shape[0], rank // n_tp), BF16),
            like(wk),
            like(kvg),
            pltpu.VMEM((n_kv, wuk.shape[0], LANES), BF16),
            pltpu.VMEM((n_kv,) + wuv.shape, BF16),
            like(wo),
            like(cache),
            like(rope),
            pltpu.VMEM((seqs, LANES), F32),
            pltpu.VMEM((n_kv, seqs, 2 * LANES), F32),
            pltpu.VMEM((n_kv, seqs, 2 * LANES), F32),
            pltpu.VMEM((n_kv, seqs, rank // n_tp), F32),
            pltpu.VMEM((n_tp, seqs, rank // n_tp), F32),
            pltpu.VMEM((CHUNKS, n_kv, heads // n_kv * seqs // CHUNKS, rank), BF16),
            pltpu.VMEM((n_kv, seqs, LANES), BF16),
            pltpu.VMEM((CHUNKS, n_kv, seqs // CHUNKS, wuv.shape[1]), BF16),
            pltpu.VMEM((CHUNKS, n_kv, seqs // CHUNKS, LANES), F32),
            pltpu.VMEM((seqs, half), BF16),
            pltpu.VMEM((seqs, half), BF16),
            pltpu.VMEM((seqs * heads // CHUNKS, cache.shape[1]), F32),
            pltpu.SemaphoreType.DMA((12,)),
            pltpu.SemaphoreType.DMA((5 + 3 * CHUNKS, n_kv - 1)),
            pltpu.SemaphoreType.DMA((5 + 3 * CHUNKS, n_kv)),
            pltpu.SemaphoreType.DMA((n_dp - 1, n_kv - 1)),
            pltpu.SemaphoreType.DMA((n_dp, n_kv - 1)),
            pltpu.SemaphoreType.DMA((4,)),
        ],
        compiler_params=pltpu.CompilerParams(collective_id=0, has_side_effects=True),
    )(lengths, freq, x, gain, wqn, wqr, wl, wk, kvg, wuk, wuv, wo, cache, rope)
    return pl.pallas_call(
        hand_out,
        out_shape=tuple(jax.ShapeDtypeStruct(o.shape, o.dtype) for o in outs),
        in_specs=[any_spec] * len(outs),
        out_specs=(any_spec,) * len(outs),
        scratch_shapes=[like(o) for o in outs] + [pltpu.SemaphoreType.DMA((2, len(outs)))],
    )(*outs)


def local(
    token_state,
    norm_gain,
    wq_nope,
    wq_rope,
    w_latent,
    w_rope_key,
    kv_gain,
    w_uk,
    w_uv,
    w_out,
    latent_cache,
    rope_cache,
    lengths,
):
    x_wide = token_state.astype(jnp.float32)
    scaled = (x_wide * norm_gain).astype(jnp.bfloat16)
    partials = (
        jnp.sum(x_wide * x_wide, axis=1),
        jnp.dot(scaled, wq_nope, preferred_element_type=jnp.float32),
        jnp.dot(scaled, wq_rope, preferred_element_type=jnp.float32),
        jnp.dot(scaled, w_latent, preferred_element_type=jnp.float32),
        jnp.dot(scaled, w_rope_key, preferred_element_type=jnp.float32),
    )
    squares, nope_sum, rope_sum, latent_sum, key_sum = lax.psum(
        (partials[0], partials[1], partials[2], partials[3], partials[4]), "kv"
    )
    inv_rms = lax.rsqrt(squares / D + EPS)[:, None]
    seq_count = token_state.shape[0]
    head_count = wq_nope.shape[1] // NOPE
    latent_raw = latent_sum * inv_rms
    latent_new = (
        latent_raw
        * lax.rsqrt(jnp.mean(latent_raw * latent_raw, axis=1, keepdims=True) + EPS)
        * kv_gain
    ).astype(jnp.bfloat16)
    angles = rope_angles(lengths)
    rope_new = rotate(key_sum * inv_rms, angles).astype(jnp.bfloat16)
    q_rot = rotate(
        (rope_sum * inv_rms).reshape(seq_count, head_count, ROPE), angles[:, None, :]
    ).astype(jnp.bfloat16)
    q_low = (nope_sum * inv_rms).astype(jnp.bfloat16).reshape(seq_count, head_count, NOPE)
    row_count = w_uk.shape[0]
    q_piece = jnp.einsum(
        "bhn,rhn->bhr",
        q_low,
        w_uk.reshape(row_count, head_count, NOPE),
        preferred_element_type=jnp.float32,
    ).astype(jnp.bfloat16)
    q_latent = lax.all_gather(q_piece, "kv", axis=2, tiled=True)
    block_len = latent_cache.shape[1]
    positions = lax.axis_index("kv") * block_len + jnp.arange(block_len, dtype=jnp.int32)
    score_scale = (NOPE + ROPE) ** (-0.5)
    cached = jnp.einsum("bhr,bpr->bhp", q_latent, latent_cache, preferred_element_type=jnp.float32)
    cached = cached + jnp.einsum(
        "bhk,bkp->bhp", q_rot, rope_cache, preferred_element_type=jnp.float32
    )
    own = jnp.einsum("bhr,br->bh", q_latent, latent_new, preferred_element_type=jnp.float32)
    own = own + jnp.einsum("bhk,bk->bh", q_rot, rope_new, preferred_element_type=jnp.float32)
    limit = lengths[:, None, None]
    newslot = positions[None, None, :] == limit
    usable = (positions[None, None, :] < limit) | newslot
    scores = jnp.where(newslot, own[:, :, None], cached) * score_scale
    masked = jnp.where(usable, scores, NEG)
    local_max = jnp.max(masked, axis=2)
    weights = jnp.where(usable, jnp.exp(masked - local_max[..., None]), 0.0)
    totals = jnp.sum(weights, axis=2)
    rounded = weights.astype(jnp.bfloat16)
    cache_weights = jnp.where(newslot, jnp.zeros_like(rounded), rounded)
    weighted = jnp.einsum(
        "bhp,bpr->bhr", cache_weights, latent_cache, preferred_element_type=jnp.float32
    )
    own_low = lax.optimization_barrier(jnp.where(newslot, rounded, jnp.zeros_like(rounded)))
    own_weight = jnp.sum(own_low.astype(jnp.float32), axis=2)
    weighted = weighted + own_weight[..., None] * latent_new.astype(jnp.float32)[:, None, :]
    value_rows = w_uv.shape[0]
    w_values = w_uv.reshape(value_rows, head_count, V_DIM)
    highest = lax.pmax(local_max, "kv")
    factor = jnp.exp(local_max - highest)
    latent_piece = lax.psum_scatter(
        weighted * factor[..., None], "kv", scatter_dimension=2, tiled=True
    ).astype(jnp.bfloat16)
    partial_values = jnp.einsum(
        "bhr,rhv->bhv", latent_piece, w_values, preferred_element_type=jnp.float32
    )
    value_sum, totals = lax.psum((partial_values, totals * factor), "kv")
    values = value_sum / totals[:, :, None]
    attended = values.astype(jnp.bfloat16).reshape(seq_count, head_count * V_DIM)
    out_term = jnp.dot(attended, w_out, preferred_element_type=jnp.float32)
    mixed = lax.psum_scatter(out_term.astype(jnp.bfloat16), "tp", scatter_dimension=1, tiled=True)
    return (mixed, latent_new, rope_new)


def solution(mesh):
    n_dp, n_kv, n_tp = mesh.shape["dp"], mesh.shape["kv"], mesh.shape["tp"]

    def body(*args):
        width, rank = args[9].shape[1], args[4].shape[1]
        aligned = (width // n_tp) % LANES == 0 and (rank // n_kv) % LANES == 0
        if aligned and args[2].shape[1] == n_kv * LANES and n_tp == 2:
            return fused(n_dp, n_kv, n_tp, *args)
        return local(*args)

    return jax.shard_map(
        body,
        mesh=mesh,
        in_specs=(
            P("dp", "kv"),
            P("kv"),
            P("kv", "tp"),
            P("kv", "tp"),
            P("kv", None),
            P("kv", None),
            P(),
            P("kv", "tp"),
            P("kv", "tp"),
            P("tp", "kv"),
            P("dp", "kv", None),
            P("dp", None, "kv"),
            P("dp"),
        ),
        out_specs=(P("dp", ("kv", "tp")), P("dp", None), P("dp", None)),
        check_vma=False,
    )
```

```python
import functools

import jax
import jax.numpy as jnp
import numpy as np
from jax import lax
from jax.experimental import pallas as pl
from jax.experimental.pallas import tpu as pltpu
from jax.sharding import PartitionSpec as P

D = 4096
NOPE = 64
ROPE = 32
V_DIM = 64


EPS = 1e-06
THETA = 10000.0
NEG = -1e30
LANES = 128
CHUNKS = 2
MESH = pl.DeviceIdType.MESH
BF16 = jnp.bfloat16
F32 = jnp.float32


def rotate(vector, angles):
    half_dim = vector.shape[-1] // 2
    cosine = jnp.cos(angles)
    sine_part = jnp.sin(angles)
    leading = vector[..., :half_dim]
    trailing = vector[..., half_dim:]
    return jnp.concatenate(
        [leading * cosine - trailing * sine_part, trailing * cosine + leading * sine_part], axis=-1
    )


def rope_angles(lengths):
    half_dim = ROPE // 2
    inv_freq = THETA ** (-jnp.arange(half_dim, dtype=jnp.float32) * 2.0 / ROPE)
    return lengths.astype(jnp.float32)[:, None] * inv_freq[None, :]


def dot_nt(a, b):
    return lax.dot_general(a, b, (((1,), (1,)), ((), ())), preferred_element_type=F32)


def dot(a, b):
    return jnp.dot(a, b, preferred_element_type=F32)


def swap_halves(u):
    width = u.shape[1]
    half = ROPE // 2
    lane = lax.broadcasted_iota(jnp.int32, u.shape, 1)
    from_above = pltpu.roll(u, width - half, 1)
    from_below = pltpu.roll(u, half, 1)
    return jnp.where(lane % ROPE < half, -from_above, from_below)


def kernel(
    n_dp,
    n_kv,
    n_tp,
    len_ref,
    freq_ref,
    x_hbm,
    gain_hbm,
    wqn_hbm,
    wqr_hbm,
    wl_hbm,
    wk_hbm,
    kvg_hbm,
    wuk_hbm,
    wuv_hbm,
    wo_hbm,
    cache_hbm,
    rope_hbm,
    mixed_ref,
    lnew_ref,
    rnew_ref,
    x,
    gain,
    wqn,
    wqr,
    wl,
    wk,
    kvg,
    wuk,
    wuv,
    wo,
    cache,
    rope,
    key_pad,
    q_out,
    q_in,
    lat_in,
    lat_half,
    q_lat,
    q_rots,
    val_in,
    stat_in,
    half_out,
    half_in,
    scores,
    load_sem,
    send_sem,
    recv_sem,
    dp_send,
    dp_recv,
    tp_sem,
):
    me = lax.axis_index("kv")
    core = lax.axis_index("tp")
    group = lax.axis_index("dp")
    seqs = x.shape[0]
    heads = wqn.shape[1] // NOPE
    own_heads = heads // n_kv
    rank = kvg.shape[1]
    lat_cols = wl.shape[1]
    block = cache.shape[1]
    rows = wuv_hbm.shape[0]
    chunks = q_lat.shape[0]
    span = seqs // chunks
    count = span * heads
    part = rows // n_dp

    def cols(index, width):
        return pl.ds(pl.multiple_of(index * width, width), width)

    barrier = pltpu.get_barrier_semaphore()
    axes = (("kv", me, n_kv), ("tp", core, n_tp), ("dp", group, n_dp))
    for name, index, size in axes:
        for j in range(1, size):
            pl.semaphore_signal(
                barrier, inc=1, device_id={name: lax.rem(index + j, size)}, device_id_type=MESH
            )
    part_rows = cols(group, part)
    pairs = (
        (x_hbm, x),
        (gain_hbm, gain),
        (wqn_hbm, wqn),
        (wqr_hbm, wqr),
        (wk_hbm, wk),
        (wl_hbm.at[:, cols(core, lat_cols)], wl),
        (kvg_hbm, kvg),
        (wuk_hbm.at[:, cols(me, LANES)], wuk.at[me]),
        (rope_hbm, rope),
        (cache_hbm, cache),
        (wuv_hbm, wuv.at[me]),
        (wo_hbm, wo),
    )
    loads = [pltpu.make_async_copy(s, d, load_sem.at[i]) for i, (s, d) in enumerate(pairs)]
    for i in (0, 1, 4, 2, 3):
        loads[i].start()
    pl.semaphore_wait(barrier, n_kv - 1 + n_tp - 1 + n_dp - 1)

    sent = []

    def send(phase, src, dst):
        for j in range(1, n_kv):
            peer = lax.rem(me + j, n_kv)
            copy = pltpu.make_async_remote_copy(
                src_ref=src(peer),
                dst_ref=dst(me),
                send_sem=send_sem.at[phase, j - 1],
                recv_sem=recv_sem.at[phase, me],
                device_id={"kv": peer},
                device_id_type=MESH,
            )
            copy.start()
            sent.append(copy)

    def arrive(phase, dst):
        for j in range(1, n_kv):
            source = lax.rem(me + j, n_kv)
            pltpu.make_async_remote_copy(
                src_ref=dst(source),
                dst_ref=dst(source),
                send_sem=send_sem.at[phase, j - 1],
                recv_sem=recv_sem.at[phase, source],
                device_id={"kv": source},
                device_id_type=MESH,
            ).wait_recv()

    def dp_copy(which, buf, peer, j, i, owner):
        piece = buf.at[lax.rem(me + i, n_kv), cols(owner, part)]
        return pltpu.make_async_remote_copy(
            src_ref=piece,
            dst_ref=piece,
            send_sem=dp_send.at[which, j - 1, i - 1],
            recv_sem=dp_recv.at[which, owner, i - 1],
            device_id={"dp": peer},
            device_id_type=MESH,
        )

    def forward(which, phase, buf):
        arrive(phase, lambda s: buf.at[s, part_rows])
        for j in range(1, n_dp):
            for i in range(1, n_kv):
                copy = dp_copy(which, buf, lax.rem(group + j, n_dp), j, i, group)
                copy.start()
                sent.append(copy)

    def join(which, buf):
        for j in range(1, n_dp):
            owner = lax.rem(group + j, n_dp)
            for i in range(1, n_kv):
                dp_copy(which, buf, owner, j, i, owner).wait_recv()

    send(0, lambda p: wuk_hbm.at[part_rows, cols(p, LANES)], lambda s: wuk.at[s, part_rows])

    loads[0].wait()
    loads[1].wait()
    x_wide = x[...].astype(F32)
    scaled = (x_wide * gain[...]).astype(BF16)
    squares = jnp.sum(x_wide * x_wide, axis=1, keepdims=True)
    key_pad[...] = jnp.broadcast_to(squares, key_pad.shape)
    loads[4].wait()
    key_pad[:, :ROPE] = dot_nt(scaled, wk[...])
    rope_own = own_heads * ROPE
    key_part = pltpu.roll(key_pad[...], rope_own, 1)
    loads[2].wait()
    for i in (5, 7, 6, 8, 9, 10, 11):
        loads[i].start()
    nope_part = dot(scaled, wqn[...])
    loads[3].wait()
    rope_part = dot(scaled, wqr[...])
    lane = lax.broadcasted_iota(jnp.int32, (seqs, LANES), 1)
    for s in range(n_kv):
        q_out[s, :, :LANES] = nope_part[:, s * LANES : (s + 1) * LANES]
        first, shift = divmod(s * rope_own, LANES)
        piece = rope_part[:, first * LANES : (first + 1) * LANES]
        if shift:
            piece = pltpu.roll(piece, LANES - shift, 1)
        q_out[s, :, LANES:] = jnp.where(lane < rope_own, piece, key_part)
    send(1, lambda p: q_out.at[p], lambda s: q_in.at[s])
    q_in[me] = q_out[me]
    send(2, lambda p: wuv_hbm.at[part_rows], lambda s: wuv.at[s, part_rows])
    loads[5].wait()
    lat_in[me] = dot(scaled, wl[...])
    send(3, lambda p: lat_in.at[me], lambda s: lat_in.at[s])

    row = lax.broadcasted_iota(jnp.int32, (seqs, LANES), 0)
    length_rows = jnp.zeros((seqs, LANES), jnp.int32)
    for b in range(seqs):
        length_rows = jnp.where(row == b, len_ref[b], length_rows)
    angles = length_rows.astype(F32) * freq_ref[...]
    cosine = jnp.cos(angles)
    sine = jnp.sin(angles)

    forward(0, 0, wuk)
    arrive(1, lambda s: q_in.at[s])
    total_q = q_in[0]
    for s in range(1, n_kv):
        total_q = total_q + q_in[s]
    last = total_q[:, LANES:]
    inv_rms = lax.rsqrt(last[:, LANES - 1 :] / D + EPS)
    q_low = total_q[:, :LANES] * inv_rms
    last = last * inv_rms
    turned = (last * cosine + swap_halves(last) * sine).astype(BF16)
    q_rots[me] = turned
    send(4, lambda p: q_rots.at[me], lambda s: q_rots.at[s])
    q_blocks = jnp.concatenate(
        [
            jnp.where(lane[:span] // NOPE == h, q_low[c * span : (c + 1) * span], 0.0)
            for c in range(chunks)
            for h in range(own_heads)
        ],
        axis=0,
    ).astype(BF16)
    loads[7].wait()
    join(0, wuk)
    per_chunk = own_heads * span
    for s in range(n_kv):
        piece = dot_nt(q_blocks, wuk[s]).astype(BF16)
        for c in range(chunks):
            q_lat[c, me, :, s * rows : (s + 1) * rows] = piece[c * per_chunk : (c + 1) * per_chunk]
    for c in range(chunks):
        send(5 + c, lambda p: q_lat.at[c, me], lambda s: q_lat.at[c, s])
    rope_new = pltpu.roll(turned.astype(F32), LANES - rope_own, 1)
    rnew_ref[...] = rope_new[:, :ROPE].astype(BF16)

    forward(1, 2, wuv)

    arrive(3, lambda s: lat_in.at[s])
    total_l = lat_in[0]
    for s in range(1, n_kv):
        total_l = total_l + lat_in[s]
    lat_half[core] = total_l
    other = lax.rem(core + 1, n_tp)
    lat_swap = pltpu.make_async_remote_copy(
        src_ref=lat_half.at[core],
        dst_ref=lat_half.at[core],
        send_sem=tp_sem.at[0],
        recv_sem=tp_sem.at[1],
        device_id={"tp": other},
        device_id_type=MESH,
    )
    lat_swap.start()

    arrive(4, lambda s: q_rots.at[s])
    wide = jnp.concatenate([q_rots[s] for s in range(n_kv)], axis=1).astype(F32)
    shape = (seqs, heads, n_kv * LANES)
    head = lax.broadcasted_iota(jnp.int32, shape, 1)
    at = lax.broadcasted_iota(jnp.int32, shape, 2)
    mine = (at // LANES == head // own_heads) & ((at % LANES) // ROPE == head % own_heads)
    r_blocks = jnp.where(mine, jnp.broadcast_to(wide[:, None, :], shape), 0.0)
    r_blocks = r_blocks.reshape(seqs * heads, n_kv * LANES).astype(BF16)
    pick_shape = (n_kv * LANES, LANES)
    pick = (
        lax.broadcasted_iota(jnp.int32, pick_shape, 0) % ROPE
        == lax.broadcasted_iota(jnp.int32, pick_shape, 1)
    )
    q_rot_rows = dot(r_blocks, jnp.where(pick, 1.0, 0.0).astype(BF16))

    to = lax.broadcasted_iota(jnp.int32, (count, count), 0)
    frm = lax.broadcasted_iota(jnp.int32, (count, count), 1)
    order = jnp.where(frm == (to % heads) * span + to // heads, 1.0, 0.0).astype(BF16)
    place = me * block + lax.broadcasted_iota(jnp.int32, (count, block), 1)
    score_scale = (NOPE + ROPE) ** (-0.5)
    stat_shape = (span, heads, LANES)
    stat_head = lax.broadcasted_iota(jnp.int32, stat_shape, 1)
    stat_lane = lax.broadcasted_iota(jnp.int32, stat_shape, 2)
    width = wuv.shape[2]
    val_shape = (span, heads, width)
    own_columns = lax.broadcasted_iota(jnp.int32, val_shape, 2) // V_DIM == (
        lax.broadcasted_iota(jnp.int32, val_shape, 1)
    )

    def rows_of(u):
        return jnp.broadcast_to(u[:, None, :], (span, heads, u.shape[1])).reshape(
            count, u.shape[1]
        )

    for c in range(chunks):
        first = c * span
        arrive(5 + c, lambda s: q_lat.at[c, s])
        q_latent = dot(order, q_lat[c].reshape(count, rank))
        q_turn = q_rot_rows[first * heads : (first + span) * heads]
        if c == 0:
            loads[8].wait()
            loads[9].wait()
        for b in range(span):
            some = slice(b * heads, (b + 1) * heads)
            scores[some, :] = dot_nt(q_latent[some].astype(BF16), cache[first + b]) + dot(
                q_turn[some, :ROPE].astype(BF16), rope[first + b]
            )
        if c == 0:
            loads[6].wait()
            lat_swap.wait()
            latent_raw = jnp.concatenate([lat_half[t] for t in range(n_tp)], axis=1) * inv_rms
            mean_square = jnp.mean(latent_raw * latent_raw, axis=1, keepdims=True)
            latent_new = latent_raw * lax.rsqrt(mean_square + EPS) * kvg[...]
            latent_new = latent_new.astype(BF16)
            lnew_ref[...] = latent_new
            latent_wide = latent_new.astype(F32)

        new_rows = rows_of(latent_wide[first : first + span])
        key_rows = rows_of(rope_new[first : first + span])
        own = jnp.sum(q_latent * new_rows, axis=1, keepdims=True)
        own = own + jnp.sum(q_turn * key_rows, axis=1, keepdims=True)

        limit = jnp.concatenate(
            [jnp.full((heads, block), len_ref[first + b], jnp.int32) for b in range(span)], axis=0
        )
        newslot = place == limit
        usable = place <= limit
        masked = jnp.where(usable, jnp.where(newslot, own, scores[...]) * score_scale, NEG)
        local_max = jnp.max(masked, axis=1, keepdims=True)
        weights = jnp.where(usable, jnp.exp(masked - local_max), 0.0)
        totals = jnp.sum(weights, axis=1, keepdims=True)
        rounded = weights.astype(BF16).astype(F32)
        own_weight = jnp.sum(jnp.where(newslot, rounded, 0.0), axis=1, keepdims=True)
        cache_weights = jnp.where(newslot, 0.0, rounded)
        stats = jnp.where(
            stat_lane == stat_head,
            jnp.broadcast_to(local_max, (count, LANES)).reshape(stat_shape),
            0.0,
        ) + jnp.where(
            stat_lane == stat_head + LANES // 2,
            jnp.broadcast_to(totals, (count, LANES)).reshape(stat_shape),
            0.0,
        )
        stat_in[c, me] = jnp.sum(stats, axis=1)
        send(7 + c, lambda p: stat_in.at[c, me], lambda s: stat_in.at[c, s])
        weighted = jnp.concatenate(
            [
                dot(cache_weights[b * heads : (b + 1) * heads].astype(BF16), cache[first + b])
                for b in range(span)
            ],
            axis=0,
        )
        weighted = (weighted + own_weight * new_rows).astype(BF16)

        if c == 0:
            loads[10].wait()
            join(1, wuv)
        values = dot(weighted, wuv[...].reshape(rank, width)).reshape(val_shape)
        val_in[c, me] = jnp.sum(jnp.where(own_columns, values, 0.0), axis=1).astype(BF16)
        send(9 + c, lambda p: val_in.at[c, me], lambda s: val_in.at[c, s])

    at = lax.broadcasted_iota(jnp.int32, (span, width), 1)

    def spread(u):
        out = jnp.broadcast_to(u[:, :1], (span, width))
        for h in range(1, heads):
            out = jnp.where(at // V_DIM == h, u[:, h : h + 1], out)
        return out

    merged_chunks = []
    for c in range(chunks):
        arrive(7 + c, lambda s: stat_in.at[c, s])
        maxima = [stat_in[c, s] for s in range(n_kv)]
        sums = [pltpu.roll(m, LANES // 2, 1) for m in maxima]
        highest = functools.reduce(jnp.maximum, maxima)
        factors = [jnp.exp(m - highest) for m in maxima]
        whole = functools.reduce(jnp.add, [f * t for f, t in zip(factors, sums)])
        spreads = [spread(f) for f in factors]
        divisor = spread(whole)
        arrive(9 + c, lambda s: val_in.at[c, s])
        merged = val_in[c, 0].astype(F32) * spreads[0]
        for s in range(1, n_kv):
            merged = merged + val_in[c, s].astype(F32) * spreads[s]
        merged_chunks.append(merged / divisor)
    attended = jnp.concatenate(merged_chunks, axis=0).astype(BF16)

    loads[11].wait()
    out_cols = half_in.shape[1]
    half_out[...] = dot(attended, wo[:, cols(other, out_cols)]).astype(BF16)
    swap = pltpu.make_async_remote_copy(
        src_ref=half_out,
        dst_ref=half_in,
        send_sem=tp_sem.at[2],
        recv_sem=tp_sem.at[3],
        device_id={"tp": other},
        device_id_type=MESH,
    )
    swap.start()
    kept = dot(attended, wo[:, cols(core, out_cols)]).astype(BF16)
    swap.wait()
    mixed_ref[...] = (kept.astype(F32) + half_in[...].astype(F32)).astype(BF16)
    for c in sent:
        c.wait_send()


def hand_out(*refs):
    n = (len(refs) - 1) // 3
    ins, outs, held, sem = refs[:n], refs[n : 2 * n], refs[2 * n : 3 * n], refs[-1]
    for step, (frm, to) in enumerate(((ins, held), (held, outs))):
        copies = [pltpu.make_async_copy(frm[i], to[i], sem.at[step, i]) for i in range(n)]
        for copy in copies:
            copy.start()
        for copy in copies:
            copy.wait()


def fused(n_dp, n_kv, n_tp, *args):
    (x, gain, wqn, wqr, wl, wk, kvg, wuk, wuv, wo, cache, rope, lengths) = args
    seqs, rank = x.shape[0], wl.shape[1]
    heads = wqn.shape[1] // NOPE
    half = wo.shape[1] // n_tp
    freq = THETA ** (-(np.arange(LANES) % (ROPE // 2)) * 2.0 / ROPE)
    freq = jnp.asarray(freq.astype(np.float32)[None, :])
    any_spec = pl.BlockSpec(memory_space=pl.ANY)
    vmem = pl.BlockSpec(memory_space=pltpu.VMEM)

    def like(a):
        return pltpu.VMEM(a.shape, a.dtype)

    gain = gain.reshape(1, -1)
    kvg = kvg.reshape(1, -1)
    wk = wk.T
    outs = pl.pallas_call(
        functools.partial(kernel, n_dp, n_kv, n_tp),
        out_shape=(
            jax.ShapeDtypeStruct((seqs, half), BF16),
            jax.ShapeDtypeStruct((seqs, rank), BF16),
            jax.ShapeDtypeStruct((seqs, ROPE), BF16),
        ),
        in_specs=[pl.BlockSpec(memory_space=pltpu.SMEM), vmem] + [any_spec] * 12,
        out_specs=(vmem, vmem, vmem),
        scratch_shapes=[
            like(x),
            like(gain),
            like(wqn),
            like(wqr),
            pltpu.VMEM((wl.shape[0], rank // n_tp), BF16),
            like(wk),
            like(kvg),
            pltpu.VMEM((n_kv, wuk.shape[0], LANES), BF16),
            pltpu.VMEM((n_kv,) + wuv.shape, BF16),
            like(wo),
            like(cache),
            like(rope),
            pltpu.VMEM((seqs, LANES), F32),
            pltpu.VMEM((n_kv, seqs, 2 * LANES), F32),
            pltpu.VMEM((n_kv, seqs, 2 * LANES), F32),
            pltpu.VMEM((n_kv, seqs, rank // n_tp), F32),
            pltpu.VMEM((n_tp, seqs, rank // n_tp), F32),
            pltpu.VMEM((CHUNKS, n_kv, heads // n_kv * seqs // CHUNKS, rank), BF16),
            pltpu.VMEM((n_kv, seqs, LANES), BF16),
            pltpu.VMEM((CHUNKS, n_kv, seqs // CHUNKS, wuv.shape[1]), BF16),
            pltpu.VMEM((CHUNKS, n_kv, seqs // CHUNKS, LANES), F32),
            pltpu.VMEM((seqs, half), BF16),
            pltpu.VMEM((seqs, half), BF16),
            pltpu.VMEM((seqs * heads // CHUNKS, cache.shape[1]), F32),
            pltpu.SemaphoreType.DMA((12,)),
            pltpu.SemaphoreType.DMA((5 + 3 * CHUNKS, n_kv - 1)),
            pltpu.SemaphoreType.DMA((5 + 3 * CHUNKS, n_kv)),
            pltpu.SemaphoreType.DMA((2, n_dp - 1, n_kv - 1)),
            pltpu.SemaphoreType.DMA((2, n_dp, n_kv - 1)),
            pltpu.SemaphoreType.DMA((4,)),
        ],
        compiler_params=pltpu.CompilerParams(collective_id=0, has_side_effects=True),
    )(lengths, freq, x, gain, wqn, wqr, wl, wk, kvg, wuk, wuv, wo, cache, rope)
    return pl.pallas_call(
        hand_out,
        out_shape=tuple(jax.ShapeDtypeStruct(o.shape, o.dtype) for o in outs),
        in_specs=[any_spec] * len(outs),
        out_specs=(any_spec,) * len(outs),
        scratch_shapes=[like(o) for o in outs] + [pltpu.SemaphoreType.DMA((2, len(outs)))],
    )(*outs)


def local(
    token_state,
    norm_gain,
    wq_nope,
    wq_rope,
    w_latent,
    w_rope_key,
    kv_gain,
    w_uk,
    w_uv,
    w_out,
    latent_cache,
    rope_cache,
    lengths,
):
    x_wide = token_state.astype(jnp.float32)
    scaled = (x_wide * norm_gain).astype(jnp.bfloat16)
    partials = (
        jnp.sum(x_wide * x_wide, axis=1),
        jnp.dot(scaled, wq_nope, preferred_element_type=jnp.float32),
        jnp.dot(scaled, wq_rope, preferred_element_type=jnp.float32),
        jnp.dot(scaled, w_latent, preferred_element_type=jnp.float32),
        jnp.dot(scaled, w_rope_key, preferred_element_type=jnp.float32),
    )
    squares, nope_sum, rope_sum, latent_sum, key_sum = lax.psum(
        (partials[0], partials[1], partials[2], partials[3], partials[4]), "kv"
    )
    inv_rms = lax.rsqrt(squares / D + EPS)[:, None]
    seq_count = token_state.shape[0]
    head_count = wq_nope.shape[1] // NOPE
    latent_raw = latent_sum * inv_rms
    latent_new = (
        latent_raw
        * lax.rsqrt(jnp.mean(latent_raw * latent_raw, axis=1, keepdims=True) + EPS)
        * kv_gain
    ).astype(jnp.bfloat16)
    angles = rope_angles(lengths)
    rope_new = rotate(key_sum * inv_rms, angles).astype(jnp.bfloat16)
    q_rot = rotate(
        (rope_sum * inv_rms).reshape(seq_count, head_count, ROPE), angles[:, None, :]
    ).astype(jnp.bfloat16)
    q_low = (nope_sum * inv_rms).astype(jnp.bfloat16).reshape(seq_count, head_count, NOPE)
    row_count = w_uk.shape[0]
    q_piece = jnp.einsum(
        "bhn,rhn->bhr",
        q_low,
        w_uk.reshape(row_count, head_count, NOPE),
        preferred_element_type=jnp.float32,
    ).astype(jnp.bfloat16)
    q_latent = lax.all_gather(q_piece, "kv", axis=2, tiled=True)
    block_len = latent_cache.shape[1]
    positions = lax.axis_index("kv") * block_len + jnp.arange(block_len, dtype=jnp.int32)
    score_scale = (NOPE + ROPE) ** (-0.5)
    cached = jnp.einsum("bhr,bpr->bhp", q_latent, latent_cache, preferred_element_type=jnp.float32)
    cached = cached + jnp.einsum(
        "bhk,bkp->bhp", q_rot, rope_cache, preferred_element_type=jnp.float32
    )
    own = jnp.einsum("bhr,br->bh", q_latent, latent_new, preferred_element_type=jnp.float32)
    own = own + jnp.einsum("bhk,bk->bh", q_rot, rope_new, preferred_element_type=jnp.float32)
    limit = lengths[:, None, None]
    newslot = positions[None, None, :] == limit
    usable = (positions[None, None, :] < limit) | newslot
    scores = jnp.where(newslot, own[:, :, None], cached) * score_scale
    masked = jnp.where(usable, scores, NEG)
    local_max = jnp.max(masked, axis=2)
    weights = jnp.where(usable, jnp.exp(masked - local_max[..., None]), 0.0)
    totals = jnp.sum(weights, axis=2)
    rounded = weights.astype(jnp.bfloat16)
    cache_weights = jnp.where(newslot, jnp.zeros_like(rounded), rounded)
    weighted = jnp.einsum(
        "bhp,bpr->bhr", cache_weights, latent_cache, preferred_element_type=jnp.float32
    )
    own_low = lax.optimization_barrier(jnp.where(newslot, rounded, jnp.zeros_like(rounded)))
    own_weight = jnp.sum(own_low.astype(jnp.float32), axis=2)
    weighted = weighted + own_weight[..., None] * latent_new.astype(jnp.float32)[:, None, :]
    value_rows = w_uv.shape[0]
    w_values = w_uv.reshape(value_rows, head_count, V_DIM)
    highest = lax.pmax(local_max, "kv")
    factor = jnp.exp(local_max - highest)
    latent_piece = lax.psum_scatter(
        weighted * factor[..., None], "kv", scatter_dimension=2, tiled=True
    ).astype(jnp.bfloat16)
    partial_values = jnp.einsum(
        "bhr,rhv->bhv", latent_piece, w_values, preferred_element_type=jnp.float32
    )
    value_sum, totals = lax.psum((partial_values, totals * factor), "kv")
    values = value_sum / totals[:, :, None]
    attended = values.astype(jnp.bfloat16).reshape(seq_count, head_count * V_DIM)
    out_term = jnp.dot(attended, w_out, preferred_element_type=jnp.float32)
    mixed = lax.psum_scatter(out_term.astype(jnp.bfloat16), "tp", scatter_dimension=1, tiled=True)
    return (mixed, latent_new, rope_new)


def solution(mesh):
    n_dp, n_kv, n_tp = mesh.shape["dp"], mesh.shape["kv"], mesh.shape["tp"]

    def body(*args):
        width, rank = args[9].shape[1], args[4].shape[1]
        aligned = (width // n_tp) % LANES == 0 and (rank // n_kv) % LANES == 0
        if aligned and args[2].shape[1] == n_kv * LANES and n_tp == 2:
            return fused(n_dp, n_kv, n_tp, *args)
        return local(*args)

    return jax.shard_map(
        body,
        mesh=mesh,
        in_specs=(
            P("dp", "kv"),
            P("kv"),
            P("kv", "tp"),
            P("kv", "tp"),
            P("kv", None),
            P("kv", None),
            P(),
            P("kv", "tp"),
            P("kv", "tp"),
            P("tp", "kv"),
            P("dp", "kv", None),
            P("dp", None, "kv"),
            P("dp"),
        ),
        out_specs=(P("dp", ("kv", "tp")), P("dp", None), P("dp", None)),
        check_vma=False,
    )
```
